32 devices in a mesh: sp: 8 (over z, x), tp: 4 (over y, core).
Axes of the slice: x: 2, y: 2, z: 4, core: 2. Of those that a mesh axis runs over, the one named last changes fastest.
Arguments:
- queries: bfloat16 [2048, 1024], P('sp', 'tp'), may hold values from -64 to 64
- keys: bfloat16 [2048, 1024], P('sp', 'tp'), may hold values from -64 to 64
- values: bfloat16 [2048, 1024], P('sp', 'tp'), may hold values from -6 to 6
- cum_gate: float32 [16, 2048], P('tp'), may hold values from -2048 to 0, as said below
- out_weight: bfloat16 [1024, 2048], P('tp'), may hold values from -0.375 to 0.375
- resid: bfloat16 [2048, 2048], P('sp'), may hold values from -6 to 6
- norm_gain: float32 [2048], replicated, may hold values from 0.1 to 1.9
- routes: int32 [2048, 2], P('sp'), may hold values from 0 to 7, all different within a row; in each aligned block of 256 rows (0 to 255, 256 to 511, ...) at most 80 rows name the same one
- route_weight: float32 [2048, 2], P('sp'), may hold values from 0.1 to 0.9
- gate_weight: bfloat16 [8, 2048, 4096], P('sp', None, 'tp'), may hold values from -0.125 to 0.125
- up_weight: bfloat16 [8, 2048, 4096], P('sp', None, 'tp'), may hold values from -0.125 to 0.125
- down_weight: bfloat16 [8, 4096, 2048], P('sp', 'tp'), may hold values from -0.09375 to 0.09375
Outputs:
- layer_out: bfloat16 [2048, 2048], P('sp', 'tp')
The draws below stay inside these ranges and needn't reach their ends.
Inputs may be any that keep to these rules, and one draw needn't show every extreme that they name: `routes`: each token names 2 different experts. Among the rows of one index of sp, no expert is named more than 80 times, a bound that some block reaches. `cum_gate`: each head's row does not rise along the positions.
All inputs are finite; a program needn't handle non-finite values.
Results may differ from the reference program's by a relative error of at most 0.015.
Values may be sent and summed in bfloat16 or wider, within the bound.
A program may use at most 64 MiB of HBM per device.

```python
import math
import jax
import jax.numpy as jnp
import numpy as np
from jax import lax

D = 2048
HEADS = 16
HD = 64
FF = 4096
TOPK = 2
TOK_DEV = 256
SEQUENCE_TOKENS = 2048
EXPERTS = 8
CAP = 80
N_SP = 8
N_TP = 4


def draw_queries(key, part):
    base = jax.random.normal(jax.random.fold_in(key, 1), (SEQUENCE_TOKENS, HEADS * HD), jnp.float32)
    base = jnp.clip(base, -6.0, 6.0)
    return base.astype(jnp.bfloat16)


def draw_keys(key, part):
    base = jax.random.normal(jax.random.fold_in(key, 2), (SEQUENCE_TOKENS, HEADS * HD), jnp.float32)
    base = jnp.clip(base, -6.0, 6.0) * 2.0
    return base.astype(jnp.bfloat16)


def draw_cum_gate(key, part):
    parallel_flows = jax.random.split(jax.random.fold_in(key, 3), 6)
    order = jax.random.permutation(parallel_flows[0], HEADS)
    slow = order < HEADS // 2
    fast_rate = jnp.exp(jax.random.uniform(parallel_flows[1], (HEADS,), jnp.float32, jnp.log(1.0 / 100.0), jnp.log(1.0 / 30.0)))
    rate = jnp.where(slow, 0.8 / SEQUENCE_TOKENS, fast_rate)
    blocks = SEQUENCE_TOKENS // TOK_DEV
    block_factor = jnp.exp(jax.random.uniform(parallel_flows[2], (blocks,), jnp.float32, jnp.log(0.5), jnp.log(2.0)))
    rough = jax.random.uniform(parallel_flows[3], (HEADS, SEQUENCE_TOKENS), jnp.float32, 0.3, 1.7)
    forget_step = -rate[:, None] * jnp.repeat(block_factor, TOK_DEV)[None, :] * rough
    group_position = jax.random.randint(parallel_flows[4], (2,), 0, SEQUENCE_TOKENS)
    token_group = jnp.log(1.0 - jax.random.uniform(parallel_flows[5], (2,), jnp.float32, 0.2, 0.5))
    forget_step = forget_step.at[:, group_position].add(token_group[None, :])
    return jnp.cumsum(forget_step, axis=1)


def steps_of(stream_key, dims, pieces, smallest, largest):
    gain = 1.0
    for axis_at, blocks in pieces:
        draws = jax.random.uniform(jax.random.fold_in(jax.random.fold_in(stream_key, 6), axis_at), (blocks,), jnp.float32, smallest / len(pieces), largest / len(pieces))
        gain = gain * jnp.repeat(jnp.exp(draws), dims[axis_at] // blocks).reshape((-1,) + (1,) * (len(dims) - 1 - axis_at))
    return gain


def assign_block(rng, own, number, rows, number_of, top, bound, slope):
    ranking = jax.random.permutation(rng, number_of)
    crowded, ordinary = portions_of(number_of, rows * top, bound, slope, True), portions_of(number_of, rows * top, bound, slope, False)
    places = jnp.arange(number_of)

    def named(sizes, rotation):
        used = int((sizes > 0).sum())
        fixed = max(1, used // 4)
        shifted = fixed + (places - fixed + rotation * (used - fixed)) % max(1, number_of - fixed)
        return jnp.zeros((number_of,), jnp.int32).at[ranking[jnp.where(places < fixed, places, shifted)]].set(jnp.asarray(sizes, jnp.int32))

    sizes = jnp.where(number % 4 == 0, named(crowded, number // 4), named(ordinary, number - number // 4 - 1))
    mixed = jax.random.permutation(jax.random.fold_in(own, 3), number_of)
    giver, taker = mixed[0:number_of // 2 * 2:2], mixed[1:number_of // 2 * 2:2]
    margin = jnp.minimum(sizes[giver] - 1, bound - sizes[taker]) // 2
    margin = jnp.where((giver == ranking[0]) | (taker == ranking[0]) | (sizes[taker] == 0), 0, jnp.maximum(margin, 0))
    shifted = jax.random.randint(jax.random.fold_in(own, 4), (number_of // 2,), 0, 1 << 20) % (margin + 1)
    sizes = sizes.at[giver].add(-shifted).at[taker].add(shifted)
    items = jnp.searchsorted(jnp.cumsum(sizes), jnp.arange(rows * top), side="right").astype(jnp.int32)
    table = items.reshape(top, rows).T
    table = table[jax.random.permutation(jax.random.fold_in(own, 1), rows)]
    rotation = jax.random.randint(jax.random.fold_in(own, 2), (rows, 1), 0, top)
    return jnp.take_along_axis(table, (jnp.arange(top)[None, :] + rotation) % top, axis=1)


def portions_of(number_of, total, bound, skew, full):
    loads = [(1 << 20) // math.isqrt(standing ** skew) + 1 for standing in range(1, number_of + 1)]
    largest = bound if full else min(bound, max(-(-total // number_of), total * loads[0] // sum(loads)))
    least = 1 if total - largest >= number_of - 1 else 0
    holding, spare = [largest] + [least] * (number_of - 1), total - largest - least * (number_of - 1)
    while spare > 0:
        free = [i for i in range(1, number_of) if holding[i] < largest] or [i for i in range(1, number_of) if holding[i] < bound]
        mass, remaining = sum([loads[i] for i in free]), spare
        for i in free:
            extra = min(bound - holding[i], max(1, remaining * loads[i] // mass), spare)
            holding[i] = holding[i] + extra
            spare = spare - extra
    return np.array(holding)


def gaussian(key, extent, deviation, bound, pieces=(), kind=jnp.bfloat16):
    values = deviation * jax.random.normal(key, extent, jnp.float32)
    if pieces:
        values = values * steps_of(key, extent, pieces, -0.22, 0.18)
    return jnp.clip(values, -bound, bound).astype(kind)


def setup_inputs(seed: int = 0) -> dict:
    key_of = jax.random.split(jax.random.key(seed), 13)
    queries = draw_queries(jax.random.fold_in(key_of[12], 71), 0)
    keys = draw_keys(jax.random.fold_in(key_of[12], 71), 0)
    values = gaussian(key_of[2], (SEQUENCE_TOKENS, HEADS * HD), 1.0, 6.0, ((0, 8), (1, 4)))
    cum_gate = draw_cum_gate(jax.random.fold_in(key_of[12], 71), 0)
    out_weight = gaussian(key_of[4], (HEADS * HD, D), (2.0 / (HEADS * HD) ** 0.5), 0.375, ((0, 4),))
    resid = gaussian(key_of[5], (SEQUENCE_TOKENS, D), 1.0, 6.0, ((0, 8),))
    norm_gain = jnp.clip(1.0 + 0.18 * jax.random.normal(key_of[6], (D,), jnp.float32), 0.1, 1.9)
    routes_keys = jax.random.split(jax.random.fold_in(key_of[7], 1), SEQUENCE_TOKENS // TOK_DEV)
    routes_turns = jax.random.permutation(jax.random.fold_in(key_of[7], 3), SEQUENCE_TOKENS // TOK_DEV)
    routes = jax.vmap(lambda own, number: assign_block(jax.random.fold_in(key_of[7], 2), own, number, TOK_DEV, EXPERTS, TOPK, CAP, 2))(routes_keys, routes_turns).reshape((SEQUENCE_TOKENS, TOPK))
    route_weight = jnp.clip(0.1 + 0.79999997 * jax.random.uniform(key_of[8], (SEQUENCE_TOKENS, TOPK), jnp.float32) ** steps_of(key_of[8], (SEQUENCE_TOKENS, TOPK), ((0, 8),), -0.2, 0.2), 0.1, 0.9)
    gate_weight = gaussian(key_of[9], (EXPERTS, D, FF), D ** -0.5, 0.125, ((0, 8), (2, 4)))
    up_weight = gaussian(key_of[10], (EXPERTS, D, FF), D ** -0.5, 0.125, ((0, 8), (2, 4)))
    down_weight = gaussian(key_of[11], (EXPERTS, FF, D), FF ** -0.5, 0.09375, ((0, 8), (1, 4)))
    return dict(queries=queries, keys=keys, values=values, cum_gate=cum_gate, out_weight=out_weight, resid=resid, norm_gain=norm_gain, routes=routes, route_weight=route_weight, gate_weight=gate_weight, up_weight=up_weight, down_weight=down_weight)


epsilon = 1e-06

def attention(queries, keys, values, cum_gate):
    length = queries.shape[0]
    score_scale = HD ** (-0.5)
    query_all = queries.reshape(length, HEADS, HD).astype(jnp.float32)
    key_all = keys.reshape(length, HEADS, HD).astype(jnp.float32)
    value_all = values.reshape(length, HEADS, HD).astype(jnp.float32)
    block_rows = math.gcd(length, 256)
    key_pos = jnp.arange(length, dtype=jnp.int32)

    def one_block(block_index):
        block_first = (block_index * block_rows).astype(jnp.int32)
        query_part = lax.dynamic_slice_in_dim(query_all, block_first, block_rows, 0)
        cum_query = lax.dynamic_slice_in_dim(cum_gate, block_first, block_rows, 1)
        scores = jnp.einsum('qhd,khd->hqk', query_part, key_all) * score_scale
        scores = scores + cum_query[:, :, None] - cum_gate[:, None, :]
        query_pos = block_first + jnp.arange(block_rows, dtype=jnp.int32)
        permitted_mask = (key_pos[None, :] <= query_pos[:, None])[None]
        best_score = lax.optimization_barrier(jnp.max(jnp.where(permitted_mask, scores, -jnp.inf), axis=-1, keepdims=True))
        weights = jnp.where(permitted_mask, jnp.exp(scores - best_score), 0.0)
        weight_sum = lax.optimization_barrier(jnp.sum(weights, axis=-1))
        rounded = lax.optimization_barrier(weights.astype(jnp.bfloat16)).astype(jnp.float32)
        value_sum = jnp.einsum('hqk,khd->hqd', rounded, value_all)
        return (value_sum / weight_sum[..., None]).astype(jnp.bfloat16)
    blocks = lax.map(one_block, jnp.arange(length // block_rows, dtype=jnp.int32))
    return blocks.transpose(0, 2, 1, 3).reshape(length, HEADS * HD)

def project(attended, out_weight):
    length = attended.shape[0]
    group_cols = HEADS * HD // N_TP
    parts = attended.reshape(length, N_TP, group_cols).transpose(1, 0, 2)
    weight_parts = out_weight.reshape(N_TP, group_cols, D)

    def add_group(running, pair):
        term = jnp.dot(pair[0], pair[1], preferred_element_type=jnp.float32)
        rounded = lax.optimization_barrier(term.astype(jnp.bfloat16)).astype(jnp.float32)
        return (running + rounded, None)
    mixed_sum, ignored = lax.scan(add_group, jnp.zeros((length, D), jnp.float32), (parts, weight_parts))
    return mixed_sum

def experts_out(normed, routes, route_weight, gate_weight, up_weight, down_weight):
    length = normed.shape[0]
    capacity = N_SP * CAP
    chosen = routes.reshape(-1).astype(jnp.int32)
    row_of = jnp.arange(length * TOPK, dtype=jnp.int32) // TOPK
    weight_flat = route_weight.reshape(-1)
    group_rows = FF // N_TP

    def add_expert(running, expert_index):
        hit = (chosen == expert_index).astype(jnp.int32)
        rank_within = jnp.cumsum(hit) - hit
        slot_index = jnp.where(hit > 0, rank_within, capacity).astype(jnp.int32)
        source_row = jnp.zeros((capacity + 1,), jnp.int32).at[slot_index].set(row_of)[:capacity]
        slot_weight = jnp.zeros((capacity + 1,), jnp.float32).at[slot_index].set(weight_flat * hit.astype(jnp.float32))[:capacity]
        arrived_rows = normed[source_row]
        gate_sum = jnp.dot(arrived_rows, gate_weight[expert_index], preferred_element_type=jnp.float32)
        up_sum = jnp.dot(arrived_rows, up_weight[expert_index], preferred_element_type=jnp.float32)
        hidden = (jax.nn.silu(gate_sum) * up_sum).astype(jnp.bfloat16)
        hidden_groups = hidden.reshape(capacity, N_TP, group_rows).transpose(1, 0, 2).astype(jnp.float32)
        down_groups = down_weight[expert_index].reshape(N_TP, group_rows, D).astype(jnp.float32)
        terms = jnp.einsum('grf,gfd->grd', hidden_groups, down_groups)
        rounded = lax.optimization_barrier(terms.astype(jnp.bfloat16)).astype(jnp.float32)
        expert_rows = lax.optimization_barrier(jnp.sum(rounded, axis=0)).astype(jnp.bfloat16)
        running = running.at[source_row].add(slot_weight[:, None] * expert_rows.astype(jnp.float32))
        return (running, None)
    combined, ignored = lax.scan(add_expert, jnp.zeros((length, D), jnp.float32), jnp.arange(EXPERTS, dtype=jnp.int32))
    return combined

def reference(queries, keys, values, cum_gate, out_weight, resid, norm_gain, routes, route_weight, gate_weight, up_weight, down_weight):
    attended = attention(queries, keys, values, cum_gate)
    stream = resid.astype(jnp.float32) + project(attended, out_weight)
    square_mean = lax.optimization_barrier(jnp.mean(stream * stream, axis=1, keepdims=True))
    normed = (stream * lax.rsqrt(square_mean + epsilon) * norm_gain).astype(jnp.bfloat16)
    combined = experts_out(normed, routes, route_weight, gate_weight, up_weight, down_weight)
    return (stream + combined).astype(jnp.bfloat16)
```

```python
import functools

import jax
import jax.numpy as jnp
from jax import lax
from jax.experimental import pallas as pl
from jax.experimental.pallas import tpu as pltpu
from jax.sharding import PartitionSpec as P

HD = 64
LANES = 128
EPSILON = 1e-06
MESH = pl.DeviceIdType.MESH
VMEM_BYTES = 60 * 1024 * 1024


def remote(src, dst, send_sem, recv_sem, s, t):
    return pltpu.make_async_remote_copy(
        src_ref=src,
        dst_ref=dst,
        send_sem=send_sem,
        recv_sem=recv_sem,
        device_id=(s, t),
        device_id_type=MESH,
    )


def offset_of(d, sp):
    half = sp // 2
    low, top = (d // 2) % 2, d // half
    return d - 2 * low - half * top + half * low + 2 * top


def greet(sp, tp, s, t):
    barrier = pltpu.get_barrier_semaphore()
    for d in range(1, sp):
        pl.semaphore_signal(barrier, inc=1, device_id=(s ^ d, t), device_id_type=MESH)
    for a in range(1, tp):
        pl.semaphore_signal(barrier, inc=1, device_id=(s, t ^ a), device_id_type=MESH)
    pl.semaphore_wait(barrier, sp + tp - 2)


class Gather:
    def __init__(self, buf, y_send, p_send, recv, s, t, tp):
        self.buf, self.y_send, self.p_send, self.recv = buf, y_send, p_send, recv
        self.s, self.t, self.ny = s, t, tp // 2

    def y_copy(self, k):
        at = self.buf.at[self.t]
        return remote(at, at, self.y_send.at[k], self.recv.at[self.t], self.s, self.t ^ (2 * k))

    def p_copy(self, k):
        a = self.t ^ (2 * k)
        at = self.buf.at[a]
        return remote(at, at, self.p_send.at[k], self.recv.at[a], self.s, self.t ^ 1)

    def arrival(self, a):
        at = self.buf.at[a]
        return remote(at, at, self.p_send.at[0], self.recv.at[a], self.s, self.t ^ 1)

    def start(self):
        for k in range(1, self.ny):
            self.y_copy(k).start()
        self.p_copy(0).start()

    def relay(self):
        for k in range(1, self.ny):
            self.arrival(self.t ^ (2 * k)).wait_recv()
            self.p_copy(k).start()

    def finish(self):
        for k in range(self.ny):
            self.arrival(self.t ^ (2 * k + 1)).wait_recv()

    def drain(self):
        for k in range(1, self.ny):
            self.y_copy(k).wait_send()
        for k in range(self.ny):
            self.p_copy(k).wait_send()


def attend_kernel(
    sp, tp, hpd, q_ref, kv_ref, cq_ref, ck_ref, w_ref, resid_ref, gain_ref, pick_ref,
    stream_out, rows_out,
    qbuf, kvbuf, osend, obuf, wbuf, attbuf, stream, normed,
    q_send, q_recv, kv_send, kv_recv, o_send, o_recv, local_sem,
    wy_send, wp_send, w_recv, ay_send, ap_send, a_recv,
):
    s, t = lax.axis_index("sp"), lax.axis_index("tp")
    g = sp // hpd
    piece = q_ref.shape[1]
    rows = kv_ref.shape[1]
    cols = stream_out.shape[1]
    own_w = pltpu.make_async_copy(w_ref, wbuf.at[t], local_sem.at[0])
    own_w.start()
    own_q = pltpu.make_async_copy(q_ref.at[s], qbuf.at[s], local_sem.at[1])
    own_q.start()
    own_kv = pltpu.make_async_copy(kv_ref.at[s // g], kvbuf.at[s], local_sem.at[2])
    own_kv.start()
    greet(sp, tp, s, t)

    def q_copy(d):
        dst = s ^ d
        return remote(q_ref.at[dst], qbuf.at[s], q_send.at[d], q_recv.at[s], dst, t)

    def kv_copy(d):
        dst = s ^ d
        return remote(kv_ref.at[dst // g], kvbuf.at[s], kv_send.at[d], kv_recv.at[s], dst, t)

    for d in range(sp - 1, 0, -1):
        kv_copy(d).start()
        q_copy(d).start()
    own_w.wait()
    w_gather = Gather(wbuf, wy_send, wp_send, w_recv, s, t, tp)
    w_gather.start()
    own_q.wait()
    own_kv.wait()
    first = lax.rem(s, g) * piece

    def o_copy(i):
        return remote(osend.at[i], obuf.at[s], o_send.at[i], o_recv.at[s], i, t)

    for i in range(sp):
        @pl.when(s != i)
        def _():
            remote(qbuf.at[i], qbuf.at[i], q_send.at[0], q_recv.at[i], s ^ 1, t).wait_recv()
            remote(kvbuf.at[i], kvbuf.at[i], kv_send.at[0], kv_recv.at[i], s ^ 1, t).wait_recv()

        q = qbuf[i]
        cq = cq_ref[i]
        kv_here = kvbuf[i]
        contract = (((1,), (1,)), ((), ()))
        diag = lax.dot_general(q, kv_here, contract, preferred_element_type=jnp.float32)
        diag = diag + cq - ck_ref[:, i * rows:(i + 1) * rows]
        qpos = first + lax.broadcasted_iota(jnp.int32, diag.shape, 0)
        kpos = lax.broadcasted_iota(jnp.int32, diag.shape, 1)
        diag = jnp.where(kpos <= qpos, diag, -jnp.inf)
        best = jnp.max(diag, axis=1, keepdims=True)
        if i:
            kv_past = kvbuf[0:i].reshape(i * rows, LANES)
            past = lax.dot_general(q, kv_past, contract, preferred_element_type=jnp.float32)
            past = past + cq - ck_ref[:, :i * rows]
            best = jnp.maximum(best, jnp.max(past, axis=1, keepdims=True))
        weights = jnp.exp(diag - best)
        total = jnp.sum(weights, axis=1, keepdims=True)
        value = jnp.dot(weights.astype(jnp.bfloat16), kv_here, preferred_element_type=jnp.float32)
        if i:
            weights = jnp.exp(past - best)
            total = total + jnp.sum(weights, axis=1, keepdims=True)
            value = value + jnp.dot(
                weights.astype(jnp.bfloat16), kv_past, preferred_element_type=jnp.float32
            )
        osend[i] = (value / total).astype(jnp.bfloat16)

        @pl.when(s != i)
        def _():
            o_copy(i).start()

        @pl.when(s == i)
        def _():
            obuf[i] = osend[i]

    w_gather.relay()
    for d in range(1, sp):
        j = s ^ d
        remote(obuf.at[j], obuf.at[j], o_send.at[0], o_recv.at[j], j, t).wait_recv()
    for r in range(g):
        part = pl.ds(r * piece, piece)
        if hpd == 1:
            attbuf[t, part, :] = obuf[r][:, :HD]
        else:
            low = lax.broadcasted_iota(jnp.int32, (piece, LANES), 1) < HD
            for p in range(hpd // 2):
                even = obuf[(2 * p) * g + r].astype(jnp.float32)
                odd = obuf[(2 * p + 1) * g + r].astype(jnp.float32)
                attbuf[t, part, p * LANES:(p + 1) * LANES] = jnp.where(low, even, odd).astype(jnp.bfloat16)
    a_gather = Gather(attbuf, ay_send, ap_send, a_recv, s, t, tp)
    a_gather.start()
    a_gather.relay()
    w_gather.finish()
    a_gather.finish()
    mixed = resid_ref[...].astype(jnp.float32)
    for a in range(tp):
        mixed = mixed + jnp.dot(attbuf[a], wbuf[a], preferred_element_type=jnp.float32)
    stream[...] = mixed
    square = jnp.mean(mixed * mixed, axis=1, keepdims=True)
    mine = pl.ds(pl.multiple_of(t * cols, cols), cols)
    here = stream[:, mine]
    stream_out[...] = here
    normed[...] = (here * lax.rsqrt(square + EPSILON) * gain_ref[:, mine]).astype(jnp.bfloat16)
    rows_out[...] = jnp.dot(
        pick_ref[...], normed[...], preferred_element_type=jnp.float32
    ).astype(jnp.bfloat16)
    for d in range(1, sp):
        q_copy(d).wait_send()
        kv_copy(d).wait_send()
    for i in range(sp):
        @pl.when(s != i)
        def _():
            o_copy(i).wait_send()
    w_gather.drain()
    a_gather.drain()


def expert_kernel(
    sp, tp, tile, rows_ref, wg_ref, wu_ref, wd_ref, hi_ref, lo_ref, stream_ref,
    out_ref,
    gath, wg, wu, wd, hid, psend, precv, ysend, yrecv, own, erows, ret,
    w_sem, x_send, x_recv, gy_send, gp_send, g_recv,
    ps_send, ps_recv, ys_send, ys_recv, r_send, r_recv,
):
    s, t = lax.axis_index("sp"), lax.axis_index("tp")
    ny = tp // 2
    slots, cols = rows_ref.shape[1], rows_ref.shape[2]
    units = hid.shape[1]
    f32, bf16 = jnp.float32, jnp.bfloat16
    loads = [
        pltpu.make_async_copy(src, dst, w_sem.at[i])
        for i, (src, dst) in enumerate(((wg_ref, wg), (wu_ref, wu), (wd_ref, wd)))
    ]

    def window(a):
        return pl.ds(pl.multiple_of(a * cols, cols), cols)

    own_rows = pltpu.make_async_copy(rows_ref.at[0], gath.at[0, :, window(t)], w_sem.at[3])
    own_rows.start()
    greet(sp, tp, s, t)

    def x_copy(d):
        return remote(
            rows_ref.at[d], gath.at[d, :, window(t)], x_send.at[d], x_recv.at[d], s ^ offset_of(d, sp), t
        )

    for d in range(1, sp):
        x_copy(d).start()
    for load in loads:
        load.start()

    def y_copy(d, k):
        at = gath.at[d, :, window(t)]
        return remote(at, at, gy_send.at[d, k], g_recv.at[d, t], s, t ^ (2 * k))

    def p_copy(d, k):
        a = t ^ (2 * k)
        at = gath.at[d, :, window(a)]
        return remote(at, at, gp_send.at[d, k], g_recv.at[d, a], s, t ^ 1)

    def arrival(d, a):
        at = gath.at[d, :, window(a)]
        return remote(at, at, gp_send.at[d, 0], g_recv.at[d, a], s, t ^ 1)

    def spread(d):
        for k in range(1, ny):
            y_copy(d, k).start()
        p_copy(d, 0).start()

    def forward(d):
        x_copy(d).wait_recv()
        spread(d)

    def relay(d):
        for k in range(1, ny):
            arrival(d, t ^ (2 * k)).wait_recv()
            p_copy(d, k).start()

    def finish(d):
        for k in range(ny):
            arrival(d, t ^ (2 * k + 1)).wait_recv()

    def ps_copy(d, k):
        return remote(psend.at[d, k], precv.at[d, k], ps_send.at[d, k], ps_recv.at[d, k], s, t ^ 1)

    def ys_copy(d, k):
        return remote(ysend.at[d, k], yrecv.at[d, k], ys_send.at[d, k], ys_recv.at[d, k], s, t ^ (2 * k))

    def r_copy(d):
        return remote(erows.at[d], ret.at[d], r_send.at[d], r_recv.at[d], s ^ offset_of(d, sp), t)

    def gate_up(d):
        x = gath[d]
        for n in range(units // tile):
            at = slice(n * tile, (n + 1) * tile)
            gate = jnp.dot(x, wg[:, at], preferred_element_type=f32)
            up = jnp.dot(x, wu[:, at], preferred_element_type=f32)
            hid[:, at] = (gate / (1.0 + jnp.exp(-gate)) * up).astype(bf16)

    order = list(range(1, ny)) + [0]

    def down(d):
        def block(b):
            return jnp.dot(hid[...], wd[:, window(b)], preferred_element_type=f32)

        for k in order:
            psend[d, k] = block(t ^ (2 * k + 1)).astype(bf16)
            ps_copy(d, k).start()
        for k in order:
            total = block(t ^ (2 * k))
            ps_copy(d, k).wait_recv()
            total = total + precv[d, k].astype(f32)
            if k:
                ysend[d, k] = total.astype(bf16)
                ys_copy(d, k).start()
            else:
                own[d] = total

    def give_back(d):
        total = own[d]
        for k in range(1, ny):
            ys_copy(d, k).wait_recv()
            total = total + yrecv[d, k].astype(f32)
        erows[d] = total.astype(bf16)

    own_rows.wait()
    spread(0)
    forward(1)
    relay(0)
    for load in loads:
        load.wait()

    def step(n, carry):
        @pl.when(n + 2 < sp)
        def _():
            forward(n + 2)

        @pl.when(n + 1 < sp)
        def _():
            relay(n + 1)

        finish(n)
        gate_up(n)
        down(n)

        @pl.when(n > 0)
        def _():
            give_back(n - 1)

            @pl.when(n > 1)
            def _():
                r_copy(n - 1).start()

        return carry

    lax.fori_loop(0, sp, step, 0)
    give_back(sp - 1)
    r_copy(sp - 1).start()
    combined = stream_ref[...]
    for d in range(sp):
        if d:
            r_copy(d).wait_recv()
        back = ret[d] if d else erows[0]
        part = slice(d * slots, (d + 1) * slots)
        combined = combined + jnp.dot(hi_ref[:, part], back, preferred_element_type=f32)
        combined = combined + jnp.dot(lo_ref[:, part], back, preferred_element_type=f32)
    out_ref[...] = combined.astype(bf16)

    def drain(d, carry):
        @pl.when(d > 0)
        def _():
            x_copy(d).wait_send()
            r_copy(d).wait_send()

        for k in range(ny):
            p_copy(d, k).wait_send()
            ps_copy(d, k).wait_send()
            if k:
                y_copy(d, k).wait_send()
                ys_copy(d, k).wait_send()
        return carry

    lax.fori_loop(0, sp, drain, 0)


def local(
    queries, keys, values, cum_gate, out_weight, resid, norm_gain, routes, route_weight,
    gate_weight, up_weight, down_weight,
):
    rows = queries.shape[0]
    hpd = queries.shape[1] // HD
    sp, tp = lax.axis_size("sp"), lax.axis_size("tp")
    s = lax.axis_index("sp")
    width = resid.shape[1]
    cols = width // tp
    g = sp // hpd
    piece = rows // g
    bf16, f32 = jnp.bfloat16, jnp.float32
    dma = pltpu.SemaphoreType.DMA

    def heads(x):
        return x.reshape(rows, hpd, HD).transpose(1, 0, 2)

    def packed(even_low, high):
        swap = (jnp.arange(hpd) % 2 == 0)[:, None, None]
        one = jnp.concatenate([even_low, high], axis=-1)
        two = jnp.concatenate([high, even_low], axis=-1)
        return jnp.where(swap, one, two)

    kv = packed(heads(values), heads(keys))
    scaled = queries * jnp.asarray(HD ** -0.5, bf16)
    q = packed(jnp.zeros((hpd, rows, HD), bf16), heads(scaled)).reshape(sp, piece, LANES)
    head_gate = lax.dynamic_slice_in_dim(cum_gate, s // g, 1, 0)
    cq = lax.dynamic_slice_in_dim(head_gate.reshape(sp, g, piece), s % g, 1, 1).reshape(sp, piece, 1)

    cap = 5 * rows // (2 * sp)
    slots = -(-cap // 16) * 16
    experts = offset_of(jnp.arange(sp, dtype=jnp.int32), sp) ^ s
    named = routes[:, :, None] == experts[None, None, :]
    count = jnp.sum(named.astype(bf16), axis=1)
    before = (jnp.arange(rows)[:, None] > jnp.arange(rows)[None, :]).astype(bf16)
    rank = jnp.dot(before, count, preferred_element_type=f32).astype(jnp.int32)
    at_rank = rank[:, :, None] == jnp.arange(slots, dtype=jnp.int32)[None, None, :]
    taken = at_rank & (count[:, :, None] > 0)
    weight = jnp.sum(jnp.where(named, route_weight[:, :, None], 0.0), axis=1)
    pick = taken.astype(bf16).transpose(1, 2, 0).reshape(sp * slots, rows)
    high = lax.reduce_precision(weight, 8, 7)
    low = weight - high
    hi = jnp.where(taken, high[:, :, None], 0.0).astype(bf16).reshape(rows, sp * slots)
    lo = jnp.where(taken, low[:, :, None], 0.0).astype(bf16).reshape(rows, sp * slots)

    vmem = pl.BlockSpec(memory_space=pltpu.VMEM)
    anywhere = pl.BlockSpec(memory_space=pl.ANY)
    ny = tp // 2
    stream_cols, outgoing = pl.pallas_call(
        functools.partial(attend_kernel, sp, tp, hpd),
        out_shape=(
            jax.ShapeDtypeStruct((rows, cols), f32),
            jax.ShapeDtypeStruct((sp * slots, cols), bf16),
        ),
        in_specs=[vmem] * 4 + [anywhere] + [vmem] * 3,
        out_specs=(vmem, vmem),
        scratch_shapes=[
            pltpu.VMEM((sp, piece, LANES), bf16),
            pltpu.VMEM((sp, rows, LANES), bf16),
            pltpu.VMEM((sp, piece, LANES), bf16),
            pltpu.VMEM((sp, piece, LANES), bf16),
            pltpu.VMEM((tp, hpd * HD, width), bf16),
            pltpu.VMEM((tp, rows, hpd * HD), bf16),
            pltpu.VMEM((rows, width), f32),
            pltpu.VMEM((rows, cols), bf16),
            dma((sp,)), dma((sp,)), dma((sp,)), dma((sp,)), dma((sp,)), dma((sp,)), dma((3,)),
            dma((ny,)), dma((ny,)), dma((tp,)), dma((ny,)), dma((ny,)), dma((tp,)),
        ],
        compiler_params=pltpu.CompilerParams(
            collective_id=0, has_side_effects=True, vmem_limit_bytes=VMEM_BYTES
        ),
        name="attend",
    )(q, kv, cq, head_gate, out_weight, resid, norm_gain[None, :], pick)

    units = gate_weight.shape[2]
    tile = min(256, units)
    return pl.pallas_call(
        functools.partial(expert_kernel, sp, tp, tile),
        out_shape=jax.ShapeDtypeStruct((rows, cols), bf16),
        in_specs=[vmem] + [anywhere] * 3 + [vmem] * 3,
        out_specs=vmem,
        scratch_shapes=[
            pltpu.VMEM((sp, slots, width), bf16),
            pltpu.VMEM((width, units), bf16),
            pltpu.VMEM((width, units), bf16),
            pltpu.VMEM((units, width), bf16),
            pltpu.VMEM((slots, units), bf16),
            pltpu.VMEM((sp, ny, slots, cols), bf16),
            pltpu.VMEM((sp, ny, slots, cols), bf16),
            pltpu.VMEM((sp, ny, slots, cols), bf16),
            pltpu.VMEM((sp, ny, slots, cols), bf16),
            pltpu.VMEM((sp, slots, cols), f32),
            pltpu.VMEM((sp, slots, cols), bf16),
            pltpu.VMEM((sp, slots, cols), bf16),
            dma((4,)), dma((sp,)), dma((sp,)), dma((sp, ny)), dma((sp, ny)), dma((sp, tp)),
            dma((sp, ny)), dma((sp, ny)), dma((sp, ny)), dma((sp, ny)), dma((sp,)), dma((sp,)),
        ],
        compiler_params=pltpu.CompilerParams(
            collective_id=1, has_side_effects=True, vmem_limit_bytes=VMEM_BYTES
        ),
        name="experts",
    )(
        outgoing.reshape(sp, slots, cols), gate_weight[0], up_weight[0], down_weight[0], hi, lo, stream_cols
    )


def solution(mesh):
    return jax.shard_map(
        local,
        mesh=mesh,
        in_specs=(
            P("sp", "tp"), P("sp", "tp"), P("sp", "tp"), P("tp", None), P("tp", None), P("sp", None),
            P(), P("sp", None), P("sp", None), P("sp", None, "tp"), P("sp", None, "tp"), P("sp", "tp", None),
        ),
        out_specs=P("sp", "tp"),
        check_vma=False,
    )
```

```python
import functools

import jax
import jax.numpy as jnp
from jax import lax
from jax.experimental import pallas as pl
from jax.experimental.pallas import tpu as pltpu
from jax.sharding import PartitionSpec as P

HD = 64
LANES = 128
EPSILON = 1e-06
MESH = pl.DeviceIdType.MESH
VMEM_BYTES = 60 * 1024 * 1024
CONTRACT_LAST = (((1,), (1,)), ((), ()))


def remote(src, dst, send_sem, recv_sem, s, t):
    return pltpu.make_async_remote_copy(
        src_ref=src,
        dst_ref=dst,
        send_sem=send_sem,
        recv_sem=recv_sem,
        device_id=(s, t),
        device_id_type=MESH,
    )


def offset_of(d, sp):
    half = sp // 2
    low, top = (d // 2) % 2, d // half
    return d - 2 * low - half * top + half * low + 2 * top


def units_of(sp):
    if sp == 8:
        return [(0, 2), (2, 1), (3, 1), (4, 2), (6, 1), (7, 1)]
    return [(d, 2) for d in range(0, sp, 2)]


def layer_kernel(
    sp, tp, hpd, slots, tile,
    q_ref, k_ref, v_ref, cum_ref, gain_ref, routes_ref, share_ref,
    w_ref, resid_ref, wg_ref, wu_ref, wd_ref,
    out_ref,
    kvs, kvbuf, qs, qbuf, osend, obuf, ckb, cqb, wbuf, attbuf, resbuf, stream, sums, pick, share,
    rows, gath, wg, wu, wd, hid, psend, precv, part, ysend, yrecv, erows, ret,
    local_sem, load_sem, kv_send, kv_relay, kv_recv, q_send, q_recv, o_send, o_recv,
    w_send, w_recv, ay_send, ap_send, a_recv, n_send, n_recv,
    x_send, x_recv, gy_send, gp_send, g_recv, ps_send, ps_recv, ys_send, ys_recv, r_send, r_recv,
):
    f32, bf16 = jnp.float32, jnp.bfloat16
    s, t = lax.axis_index("sp"), lax.axis_index("tp")
    ny = tp // 2
    g = sp // hpd
    tokens = q_ref.shape[0]
    piece = tokens // g
    packed = qs.shape[1] < piece
    short = qs.shape[1]
    width = gath.shape[2]
    cols = width // tp
    units = hid.shape[1]

    def window(a):
        return pl.ds(pl.multiple_of(a * cols, cols), cols)

    own_w = pltpu.make_async_copy(w_ref.at[:, window(t)], wbuf.at[t], local_sem.at[0])
    own_resid = pltpu.make_async_copy(resid_ref.at[:, window(t)], resbuf, local_sem.at[1])
    loads = [
        pltpu.make_async_copy(src.at[0], dst, load_sem.at[i])
        for i, (src, dst) in enumerate(((wg_ref, wg), (wu_ref, wu), (wd_ref, wd)))
    ]

    barrier = pltpu.get_barrier_semaphore()
    for d in range(1, sp):
        pl.semaphore_signal(barrier, inc=1, device_id=(s ^ d, t), device_id_type=MESH)
    for a in range(1, tp):
        pl.semaphore_signal(barrier, inc=1, device_id=(s, t ^ a), device_id_type=MESH)
    own_w.start()
    own_resid.start()

    def swap(x):
        return jnp.concatenate([x[:, HD:], x[:, :HD]], axis=1)

    def low_lanes(n):
        return lax.broadcasted_iota(jnp.int32, (n, LANES), 1) < HD

    if hpd == 1:
        kvs[0] = jnp.concatenate([v_ref[...], k_ref[...]], axis=1)
        q = q_ref[...].astype(f32) * HD ** -0.5
        q = jnp.concatenate([jnp.zeros_like(q), q], axis=1).astype(bf16)
        for j in range(sp):
            qs[j] = q[j * piece:(j + 1) * piece]
    else:
        low = low_lanes(tokens)
        for p in range(hpd // 2):
            pair = slice(p * LANES, (p + 1) * LANES)
            k = swap(k_ref[:, pair].astype(f32))
            v = v_ref[:, pair].astype(f32)
            kvs[2 * p] = jnp.where(low, v, k).astype(bf16)
            kvs[2 * p + 1] = jnp.where(low, k, v).astype(bf16)
            q = q_ref[:, pair].astype(f32) * HD ** -0.5
            turned = swap(q)
            for odd in range(2):
                for r in range(g):
                    at = r * piece
                    front = turned[at:at + short]
                    back = q[at + short:at + piece] if packed else jnp.zeros_like(front)
                    keys_low = low_lanes(short)
                    both = jnp.where(keys_low, front, back) if odd else jnp.where(keys_low, back, front)
                    qs[(2 * p + odd) * g + r] = both.astype(bf16)
    pl.semaphore_wait(barrier, sp + tp - 2)

    def kv_copy(d):
        dst = s ^ d
        return remote(kvs.at[dst // g], kvbuf.at[s], kv_send.at[d], kv_recv.at[s], dst, t)

    def kv_pass(d):
        i = s ^ d
        src = kvbuf.at[i] if d else kvs.at[s // g]
        return remote(src, kvbuf.at[i], kv_relay.at[d], kv_recv.at[i], s ^ 1, t)

    def kv_arrival(i):
        return remote(kvbuf.at[i], kvbuf.at[i], kv_relay.at[0], kv_recv.at[i], s ^ 1, t)

    def q_copy(d):
        dst = s ^ d
        return remote(qs.at[dst], qbuf.at[s], q_send.at[d], q_recv.at[s], dst, t)

    def w_copy(a):
        return remote(w_ref.at[:, window(t ^ a)], wbuf.at[t], w_send.at[a], w_recv.at[t], s, t ^ a)

    for d in range(sp - 2, 1, -2):
        kv_copy(d).start()
    kv_pass(0).start()
    for d in range(sp - 1, 0, -1):
        q_copy(d).start()
    for a in range(1, tp):
        w_copy(a).start()
    for load in loads:
        load.start()
    kvbuf[s] = kvs[s // g]
    qbuf[s] = qs[s]

    head = s // g
    first = lax.rem(s, g) * piece
    qpos = first + lax.broadcasted_iota(jnp.int32, (piece, tokens), 0)
    kpos = lax.broadcasted_iota(jnp.int32, (piece, tokens), 1)
    ckb[...] = cum_ref[pl.ds(head, 1), :]
    for i in range(sp):
        here = ckb[:, i * tokens:(i + 1) * tokens]
        cqb[i] = jnp.sum(jnp.where(kpos == qpos, here, 0.0), axis=1, keepdims=True)
    experts = offset_of(lax.broadcasted_iota(jnp.int32, (sp, tokens), 0), sp) ^ s
    chosen = [routes_ref[k:k + 1, :] == experts for k in range(2)]
    named = jnp.where(chosen[0] | chosen[1], 1.0, 0.0)
    weight = sum(jnp.where(chosen[k], share_ref[k:k + 1, :], 0.0) for k in range(2))
    high = weight.astype(bf16).astype(f32)
    parts = (high, weight - high)
    across = lax.broadcasted_iota(jnp.int32, (tokens, tokens), 1)
    along = lax.broadcasted_iota(jnp.int32, (tokens, tokens), 0)
    before = jnp.where(along < across, 1.0, 0.0).astype(bf16)
    rank = jnp.dot(named.astype(bf16), before, preferred_element_type=f32)
    rank = jnp.where(named > 0.0, rank, -1.0)
    slot = lax.broadcasted_iota(jnp.int32, (slots, tokens), 0).astype(f32)
    shares = ([], [])
    for d in range(sp):
        taken = slot == rank[d:d + 1, :]
        pick[d * slots:(d + 1) * slots, :] = jnp.where(taken, 1.0, 0.0).astype(bf16)
        for n in range(2):
            shares[n].append(jnp.where(taken, parts[n][d:d + 1, :], 0.0))
    for n in range(2):
        share[n] = jnp.concatenate(shares[n], axis=0).T.astype(bf16)

    for d in range(2, sp, 2):
        kv_arrival(s ^ d).wait_recv()
        kv_pass(d).start()

    def o_copy(i):
        return remote(osend.at[i], obuf.at[s], o_send.at[i], o_recv.at[s], i, t)

    half = lax.broadcasted_iota(jnp.int32, (short, LANES), 1) // HD
    key_lanes = (half + lax.rem(head, 2)) == 1
    for i in range(sp):
        @pl.when(s != i)
        def _():
            remote(qbuf.at[i], qbuf.at[i], q_send.at[0], q_recv.at[i], s ^ 1, t).wait_recv()

        @pl.when((s != i) & (lax.rem(s + i, 2) == 1))
        def _():
            kv_arrival(i).wait_recv()

        q = qbuf[i]
        if packed:
            q = q.astype(f32)
            q = jnp.concatenate(
                [jnp.where(key_lanes, q, 0.0), jnp.where(key_lanes, swap(q), 0.0)], axis=0
            ).astype(bf16)
        cq = cqb[i]
        kv_here = kvbuf[i]
        diag = lax.dot_general(q, kv_here, CONTRACT_LAST, preferred_element_type=f32)
        diag = diag + cq - ckb[:, i * tokens:(i + 1) * tokens]
        diag = jnp.where(kpos <= qpos, diag, -jnp.inf)
        best = jnp.max(diag, axis=1, keepdims=True)
        if i:
            kv_past = kvbuf[0:i].reshape(i * tokens, LANES)
            past = lax.dot_general(q, kv_past, CONTRACT_LAST, preferred_element_type=f32)
            past = past + cq - ckb[:, :i * tokens]
            best = jnp.maximum(best, jnp.max(past, axis=1, keepdims=True))
        weights = jnp.exp(diag - best)
        total = jnp.sum(weights, axis=1, keepdims=True)
        value = jnp.dot(weights.astype(bf16), kv_here, preferred_element_type=f32)
        if i:
            weights = jnp.exp(past - best)
            total = total + jnp.sum(weights, axis=1, keepdims=True)
            value = value + jnp.dot(weights.astype(bf16), kv_past, preferred_element_type=f32)
        value = value / total
        if packed:
            value = jnp.where(key_lanes, swap(value[short:]), value[:short])
        osend[i] = value.astype(bf16)

        @pl.when(s != i)
        def _():
            o_copy(i).start()

        @pl.when(s == i)
        def _():
            obuf[i] = osend[i]

    for d in range(1, sp):
        j = s ^ d
        remote(obuf.at[j], obuf.at[j], o_send.at[0], o_recv.at[j], j, t).wait_recv()
    low = low_lanes(short)
    for r in range(g):
        at = r * piece
        if hpd == 1:
            attbuf[t, at:at + piece, :] = obuf[r][:, :HD]
        else:
            for p in range(hpd // 2):
                pair = slice(p * LANES, (p + 1) * LANES)
                even = obuf[(2 * p) * g + r].astype(f32)
                odd = obuf[(2 * p + 1) * g + r].astype(f32)
                attbuf[t, at:at + short, pair] = jnp.where(low, even, odd).astype(bf16)
                if packed:
                    attbuf[t, at + short:at + piece, pair] = swap(jnp.where(low, odd, even)).astype(bf16)

    def ay_copy(k):
        at = attbuf.at[t]
        return remote(at, at, ay_send.at[k], a_recv.at[t], s, t ^ (2 * k))

    def ap_copy(k):
        a = t ^ (2 * k)
        at = attbuf.at[a]
        return remote(at, at, ap_send.at[k], a_recv.at[a], s, t ^ 1)

    def a_arrival(a):
        at = attbuf.at[a]
        return remote(at, at, ap_send.at[0], a_recv.at[a], s, t ^ 1)

    for k in range(1, ny):
        ay_copy(k).start()
    ap_copy(0).start()
    for k in range(1, ny):
        a_arrival(t ^ (2 * k)).wait_recv()
        ap_copy(k).start()
    own_w.wait()
    own_resid.wait()
    for a in range(1, tp):
        remote(wbuf.at[t ^ a], wbuf.at[t ^ a], w_send.at[0], w_recv.at[t ^ a], s, t ^ 1).wait_recv()
    for k in range(ny):
        a_arrival(t ^ (2 * k + 1)).wait_recv()
    mixed = resbuf[...].astype(f32)
    for a in range(tp):
        mixed = mixed + jnp.dot(attbuf[a], wbuf[a], preferred_element_type=f32)
    stream[...] = mixed
    square = jnp.sum(mixed * mixed, axis=1, keepdims=True)
    sums[t] = jnp.sum(jnp.where(along == across, square, 0.0), axis=0, keepdims=True)

    def n_copy(a):
        return remote(sums.at[t], sums.at[t], n_send.at[a], n_recv.at[t], s, t ^ a)

    for a in range(1, tp):
        n_copy(a).start()
    for a in range(1, tp):
        at = sums.at[t ^ a]
        remote(at, at, n_send.at[0], n_recv.at[t ^ a], s, t ^ 1).wait_recv()
    square = sums[0]
    for a in range(1, tp):
        square = square + sums[a]
    scale = lax.rsqrt(square / width + EPSILON)
    scale = jnp.sum(jnp.where(along == across, scale, 0.0), axis=1, keepdims=True)
    normed = (stream[...] * scale * gain_ref[:, window(t)]).astype(bf16)

    def x_copy(d):
        return remote(
            rows.at[d], gath.at[d, :, window(t)], x_send.at[d], x_recv.at[d], s ^ offset_of(d, sp), t
        )

    def y_copy(d, k):
        at = gath.at[d, :, window(t)]
        return remote(at, at, gy_send.at[d, k], g_recv.at[d, t], s, t ^ (2 * k))

    def p_copy(d, k):
        a = t ^ (2 * k)
        at = gath.at[d, :, window(a)]
        return remote(at, at, gp_send.at[d, k], g_recv.at[d, a], s, t ^ 1)

    def arrival(d, a):
        at = gath.at[d, :, window(a)]
        return remote(at, at, gp_send.at[d, 0], g_recv.at[d, a], s, t ^ 1)

    def forward(d):
        if d:
            x_copy(d).wait_recv()
        for k in range(1, ny):
            y_copy(d, k).start()
        p_copy(d, 0).start()

    def relay(d):
        for k in range(1, ny):
            arrival(d, t ^ (2 * k)).wait_recv()
            p_copy(d, k).start()

    def finish(d):
        for k in range(ny):
            arrival(d, t ^ (2 * k + 1)).wait_recv()

    def send(d, n):
        out = jnp.dot(pick[d * slots:(d + n) * slots, :], normed, preferred_element_type=f32).astype(bf16)
        for j in range(n):
            block = out[j * slots:(j + 1) * slots]
            if d + j:
                rows[d + j] = block
                x_copy(d + j).start()
            else:
                gath[0, :, window(t)] = block
                forward(0)

    pairs = [d for d in range(0, sp, 2)]
    for d in pairs[1:2] + pairs[:1] + pairs[2:]:
        send(d, 2)

    def ps_copy(d, k):
        return remote(psend.at[d, k], precv.at[d, k], ps_send.at[d, k], ps_recv.at[d, k], s, t ^ 1)

    def ys_copy(d, k):
        return remote(ysend.at[d, k], yrecv.at[d, k], ys_send.at[d, k], ys_recv.at[d, k], s, t ^ (2 * k))

    def r_copy(d):
        return remote(erows.at[d], ret.at[d], r_send.at[d], r_recv.at[d], s ^ offset_of(d, sp), t)

    def gate_up(d, n, tiles):
        x = gath[d:d + n].reshape(n * slots, width)
        for j in tiles:
            at = slice(j * tile, (j + 1) * tile)
            gate = jnp.dot(x, wg[:, at], preferred_element_type=f32)
            up = jnp.dot(x, wu[:, at], preferred_element_type=f32)
            hid[:n * slots, at] = (gate / (1.0 + jnp.exp(-gate)) * up).astype(bf16)

    order = list(range(1, ny)) + [0]

    def block(n, b):
        return jnp.dot(hid[:n * slots, :], wd[:, window(b)], preferred_element_type=f32)

    def down_pair(d, n):
        for k in order:
            out = block(n, t ^ (2 * k + 1)).astype(bf16)
            for j in range(n):
                psend[d + j, k] = out[j * slots:(j + 1) * slots]
                ps_copy(d + j, k).start()

    def down_own(d, n):
        for k in order:
            out = block(n, t ^ (2 * k))
            for j in range(n):
                part[d + j, k] = out[j * slots:(j + 1) * slots]

    def add_pair(d, n):
        for k in order:
            for j in range(n):
                ps_copy(d + j, k).wait_recv()
                total = part[d + j, k] + precv[d + j, k].astype(f32)
                if k:
                    ysend[d + j, k] = total.astype(bf16)
                    ys_copy(d + j, k).start()
                else:
                    part[d + j, k] = total

    def give_back(d, n):
        for j in range(d, d + n):
            total = part[j, 0]
            for k in range(1, ny):
                ys_copy(j, k).wait_recv()
                total = total + yrecv[j, k].astype(f32)
            erows[j] = total.astype(bf16)
            if j:
                r_copy(j).start()

    actions = [functools.partial(forward, 1)]

    def advance(limit):
        nonlocal done
        for action in actions[done:limit]:
            action()
        done = max(done, min(limit, len(actions)))

    for d in range(sp):
        if 0 < d < sp - 1:
            actions.append(functools.partial(forward, d + 1))
        actions.append(functools.partial(relay, d))
    done = 0
    work = units_of(sp)
    tiles = list(range(units // tile))
    cut = len(tiles) // 2
    loaded = False
    for n, unit in enumerate(work):
        last = unit[0] + unit[1] - 1
        advance(min(2 * last + 2, len(actions)))
        for d in range(unit[0], last + 1):
            finish(d)
        if not loaded:
            for load in loads:
                load.wait()
            loaded = True
        gate_up(*unit, tiles[:cut])
        if n:
            add_pair(*work[n - 1])
        gate_up(*unit, tiles[cut:])
        advance(done + 1)
        down_pair(*unit)
        if n > 1:
            give_back(*work[n - 2])
        down_own(*unit)
        advance(done + 1)
    add_pair(*work[-1])
    give_back(*work[-2])
    give_back(*work[-1])

    ret[0] = erows[0]
    for d in range(1, sp):
        r_copy(d).wait_recv()
    back = ret[...].reshape(sp * slots, cols)
    combined = jnp.dot(share[0], back, preferred_element_type=f32)
    combined = combined + jnp.dot(share[1], back, preferred_element_type=f32)
    combined = stream[...] + combined
    out_ref[...] = combined.astype(bf16)

    for d in range(1, sp):
        q_copy(d).wait_send()
        if d % 2 == 0:
            kv_copy(d).wait_send()
            kv_pass(d).wait_send()
    kv_pass(0).wait_send()
    for i in range(sp):
        @pl.when(s != i)
        def _():
            o_copy(i).wait_send()
    for a in range(1, tp):
        w_copy(a).wait_send()
        n_copy(a).wait_send()
    for k in range(ny):
        ap_copy(k).wait_send()
        if k:
            ay_copy(k).wait_send()

    def drain(d, carry):
        @pl.when(d > 0)
        def _():
            x_copy(d).wait_send()
            r_copy(d).wait_send()

        for k in range(ny):
            p_copy(d, k).wait_send()
            ps_copy(d, k).wait_send()
            if k:
                y_copy(d, k).wait_send()
                ys_copy(d, k).wait_send()
        return carry

    lax.fori_loop(0, sp, drain, 0)


def local(
    queries, keys, values, cum_gate, out_weight, resid, norm_gain, routes, route_weight,
    gate_weight, up_weight, down_weight,
):
    tokens = queries.shape[0]
    hpd = queries.shape[1] // HD
    sp, tp = lax.axis_size("sp"), lax.axis_size("tp")
    width = resid.shape[1]
    cols = width // tp
    units = gate_weight.shape[2]
    tile = min(256, units)
    piece = tokens // (sp // hpd)
    short = piece // 2 if hpd > 1 and piece % 32 == 0 else piece
    cap = 5 * tokens // (2 * sp)
    slots = -(-cap // 16) * 16
    ny = tp // 2
    bf16, f32 = jnp.bfloat16, jnp.float32
    dma = pltpu.SemaphoreType.DMA

    def vm(*shape, dtype=bf16):
        return pltpu.VMEM(shape, dtype)

    vmem = pl.BlockSpec(memory_space=pltpu.VMEM)
    anywhere = pl.BlockSpec(memory_space=pl.ANY)
    return pl.pallas_call(
        functools.partial(layer_kernel, sp, tp, hpd, slots, tile),
        out_shape=jax.ShapeDtypeStruct((tokens, cols), bf16),
        in_specs=[vmem] * 7 + [anywhere] * 5,
        out_specs=vmem,
        scratch_shapes=[
            vm(hpd, tokens, LANES), vm(sp, tokens, LANES),
            vm(sp, short, LANES), vm(sp, short, LANES), vm(sp, short, LANES), vm(sp, short, LANES),
            vm(1, sp * tokens, dtype=f32), vm(sp, piece, 1, dtype=f32),
            vm(tp, hpd * HD, cols), vm(tp, tokens, hpd * HD), vm(tokens, cols),
            vm(tokens, cols, dtype=f32), vm(tp, 1, tokens, dtype=f32),
            vm(sp * slots, tokens), vm(2, tokens, sp * slots),
            vm(sp, slots, cols), vm(sp, slots, width),
            vm(width, units), vm(width, units), vm(units, width), vm(2 * slots, units),
            vm(sp, ny, slots, cols), vm(sp, ny, slots, cols), vm(sp, ny, slots, cols, dtype=f32),
            vm(sp, ny, slots, cols), vm(sp, ny, slots, cols), vm(sp, slots, cols), vm(sp, slots, cols),
            dma((2,)), dma((3,)), dma((sp,)), dma((sp,)), dma((sp,)), dma((sp,)), dma((sp,)),
            dma((sp,)), dma((sp,)),
            dma((tp,)), dma((tp,)), dma((ny,)), dma((ny,)), dma((tp,)), dma((tp,)), dma((tp,)),
            dma((sp,)), dma((sp,)), dma((sp, ny)), dma((sp, ny)), dma((sp, tp)),
            dma((sp, ny)), dma((sp, ny)), dma((sp, ny)), dma((sp, ny)), dma((sp,)), dma((sp,)),
        ],
        compiler_params=pltpu.CompilerParams(
            collective_id=0, has_side_effects=True, vmem_limit_bytes=VMEM_BYTES
        ),
        name="layer",
    )(
        queries, keys, values, cum_gate, norm_gain[None, :], routes.T, route_weight.T,
        out_weight, resid, gate_weight, up_weight, down_weight,
    )


def solution(mesh):
    return jax.shard_map(
        local,
        mesh=mesh,
        in_specs=(
            P("sp", "tp"), P("sp", "tp"), P("sp", "tp"), P("tp", None), P("tp", None), P("sp", None),
            P(), P("sp", None), P("sp", None), P("sp", None, "tp"), P("sp", None, "tp"), P("sp", "tp", None),
        ),
        out_specs=P("sp", "tp"),
        check_vma=False,
    )
```

```python
import functools

import jax
import jax.numpy as jnp
from jax import lax
from jax.experimental import pallas as pl
from jax.experimental.pallas import tpu as pltpu
from jax.sharding import PartitionSpec as P

HD = 64
LANES = 128
EPSILON = 1e-06
MESH = pl.DeviceIdType.MESH
VMEM_BYTES = 60 * 1024 * 1024
CONTRACT_LAST = (((1,), (1,)), ((), ()))


def remote(src, dst, send_sem, recv_sem, s, t):
    return pltpu.make_async_remote_copy(
        src_ref=src,
        dst_ref=dst,
        send_sem=send_sem,
        recv_sem=recv_sem,
        device_id=(s, t),
        device_id_type=MESH,
    )


def layer_kernel(
    sp, tp, hpd, slots, tile,
    q_ref, k_ref, v_ref, cum_ref, gain_ref, routes_ref, share_ref,
    w_ref, resid_ref, wg_ref, wu_ref, wd_ref,
    out_ref,
    kvs, kvbuf, qs, qbuf, osend, obuf, ckb, cqb, wsrc, wbuf, attbuf, resbuf, stream, sums, pick, share,
    rows, gath, wg, wu, wd, hid, psend, precv, part, ysend, yrecv, erows, ret,
    local_sem, load_sem, kv_send, kv_relay, kv_recv, q_send, q_recv, o_send, o_recv,
    w_send, w_recv, ay_send, ap_send, a_recv, n_send, n_recv,
    x_send, x_recv, gy_send, gp_send, g_recv, ps_send, ps_recv, ys_send, ys_recv, r_send, r_recv,
):
    f32, bf16 = jnp.float32, jnp.bfloat16
    s, t = lax.axis_index("sp"), lax.axis_index("tp")
    ny = tp // 2
    g = sp // hpd
    tokens = q_ref.shape[0]
    piece = tokens // g
    packed = qs.shape[1] < piece
    short = qs.shape[1]
    width = gath.shape[2]
    cols = width // tp
    units = hid.shape[1]

    def window(a):
        return pl.ds(pl.multiple_of(a * cols, cols), cols)

    own_w = pltpu.make_async_copy(w_ref.at[:, window(t)], wbuf.at[t], local_sem.at[0])
    all_w = pltpu.make_async_copy(w_ref, wsrc, local_sem.at[2])
    own_resid = pltpu.make_async_copy(resid_ref.at[:, window(t)], resbuf, local_sem.at[1])
    loads = [
        pltpu.make_async_copy(src.at[0], dst, load_sem.at[i])
        for i, (src, dst) in enumerate(((wg_ref, wg), (wu_ref, wu), (wd_ref, wd)))
    ]

    barrier = pltpu.get_barrier_semaphore()
    for d in range(1, sp):
        pl.semaphore_signal(barrier, inc=1, device_id=(s ^ d, t), device_id_type=MESH)
    for a in range(1, tp):
        pl.semaphore_signal(barrier, inc=1, device_id=(s, t ^ a), device_id_type=MESH)
    all_w.start()
    own_w.start()
    own_resid.start()

    def swap(x):
        return jnp.concatenate([x[:, HD:], x[:, :HD]], axis=1)

    def low_lanes(n):
        return lax.broadcasted_iota(jnp.int32, (n, LANES), 1) < HD

    if hpd == 1:
        kvs[0] = jnp.concatenate([v_ref[...], k_ref[...]], axis=1)
        q = q_ref[...].astype(f32) * HD ** -0.5
        q = jnp.concatenate([jnp.zeros_like(q), q], axis=1).astype(bf16)
        for j in range(sp):
            qs[j] = q[j * piece:(j + 1) * piece]
    else:
        low = low_lanes(tokens)
        for p in range(hpd // 2):
            pair = slice(p * LANES, (p + 1) * LANES)
            k = swap(k_ref[:, pair].astype(f32))
            v = v_ref[:, pair].astype(f32)
            kvs[2 * p] = jnp.where(low, v, k).astype(bf16)
            kvs[2 * p + 1] = jnp.where(low, k, v).astype(bf16)
            q = q_ref[:, pair].astype(f32) * HD ** -0.5
            turned = swap(q)
            for odd in range(2):
                for r in range(g):
                    at = r * piece
                    front = turned[at:at + short]
                    back = q[at + short:at + piece] if packed else jnp.zeros_like(front)
                    keys_low = low_lanes(short)
                    both = jnp.where(keys_low, front, back) if odd else jnp.where(keys_low, back, front)
                    qs[(2 * p + odd) * g + r] = both.astype(bf16)
    pl.semaphore_wait(barrier, sp + tp - 2)

    def kv_copy(d):
        dst = s ^ d
        return remote(kvs.at[dst // g], kvbuf.at[s], kv_send.at[d], kv_recv.at[s], dst, t)

    def kv_pass(d):
        i = s ^ d
        src = kvbuf.at[i] if d else kvs.at[s // g]
        return remote(src, kvbuf.at[i], kv_relay.at[d], kv_recv.at[i], s ^ 1, t)

    def kv_arrival(i):
        return remote(kvbuf.at[i], kvbuf.at[i], kv_relay.at[0], kv_recv.at[i], s ^ 1, t)

    def q_copy(d):
        dst = s ^ d
        return remote(qs.at[dst], qbuf.at[s], q_send.at[d], q_recv.at[s], dst, t)

    def w_copy(a):
        return remote(wsrc.at[:, window(t ^ a)], wbuf.at[t], w_send.at[a], w_recv.at[t], s, t ^ a)

    for d in range(sp - 2, 1, -2):
        kv_copy(d).start()
    kv_pass(0).start()
    for d in range(sp - 1, 0, -1):
        q_copy(d).start()
    all_w.wait()
    for a in range(1, tp):
        w_copy(a).start()
    for load in loads:
        load.start()
    kvbuf[s] = kvs[s // g]
    qbuf[s] = qs[s]

    head = s // g
    first = lax.rem(s, g) * piece
    qpos = first + lax.broadcasted_iota(jnp.int32, (piece, tokens), 0)
    kpos = lax.broadcasted_iota(jnp.int32, (piece, tokens), 1)
    ckb[...] = cum_ref[pl.ds(head, 1), :]
    for i in range(sp):
        here = ckb[:, i * tokens:(i + 1) * tokens]
        cqb[i] = jnp.sum(jnp.where(kpos == qpos, here, 0.0), axis=1, keepdims=True)
    experts = lax.broadcasted_iota(jnp.int32, (sp, tokens), 0) ^ s
    chosen = [routes_ref[k:k + 1, :] == experts for k in range(2)]
    named = jnp.where(chosen[0] | chosen[1], 1.0, 0.0)
    weight = sum(jnp.where(chosen[k], share_ref[k:k + 1, :], 0.0) for k in range(2))
    high = weight.astype(bf16).astype(f32)
    parts = (high, weight - high)
    across = lax.broadcasted_iota(jnp.int32, (tokens, tokens), 1)
    along = lax.broadcasted_iota(jnp.int32, (tokens, tokens), 0)
    before = jnp.where(along < across, 1.0, 0.0).astype(bf16)
    rank = jnp.dot(named.astype(bf16), before, preferred_element_type=f32)
    rank = jnp.where(named > 0.0, rank, -1.0)
    slot = lax.broadcasted_iota(jnp.int32, (slots, tokens), 0).astype(f32)
    shares = ([], [])
    plan = [0] + list(range(4, sp, 2)) + [2]
    places = [d + j for d in plan for j in range(2)]
    for d in places:
        taken = slot == rank[d:d + 1, :]
        pick[d * slots:(d + 1) * slots, :] = jnp.where(taken, 1.0, 0.0).astype(bf16)
        for n in range(2):
            shares[n].append(jnp.where(taken, parts[n][d:d + 1, :], 0.0))
    for n in range(2):
        share[n] = jnp.concatenate(shares[n], axis=0).T.astype(bf16)

    for d in range(2, sp, 2):
        kv_arrival(s ^ d).wait_recv()
        kv_pass(d).start()

    def o_copy(i):
        return remote(osend.at[i], obuf.at[s], o_send.at[i], o_recv.at[s], i, t)

    half = lax.broadcasted_iota(jnp.int32, (short, LANES), 1) // HD
    key_lanes = (half + lax.rem(head, 2)) == 1
    for i in range(sp):
        @pl.when(s != i)
        def _():
            remote(qbuf.at[i], qbuf.at[i], q_send.at[0], q_recv.at[i], s ^ 1, t).wait_recv()

        @pl.when((s != i) & (lax.rem(s + i, 2) == 1))
        def _():
            kv_arrival(i).wait_recv()

        q = qbuf[i]
        if packed:
            q = q.astype(f32)
            q = jnp.concatenate(
                [jnp.where(key_lanes, q, 0.0), jnp.where(key_lanes, swap(q), 0.0)], axis=0
            ).astype(bf16)
        cq = cqb[i]
        kv_here = kvbuf[i]
        diag = lax.dot_general(q, kv_here, CONTRACT_LAST, preferred_element_type=f32)
        diag = diag + cq - ckb[:, i * tokens:(i + 1) * tokens]
        diag = jnp.where(kpos <= qpos, diag, -jnp.inf)
        best = jnp.max(diag, axis=1, keepdims=True)
        if i:
            kv_past = kvbuf[0:i].reshape(i * tokens, LANES)
            past = lax.dot_general(q, kv_past, CONTRACT_LAST, preferred_element_type=f32)
            past = past + cq - ckb[:, :i * tokens]
            best = jnp.maximum(best, jnp.max(past, axis=1, keepdims=True))
        weights = jnp.exp(diag - best)
        total = jnp.sum(weights, axis=1, keepdims=True)
        value = jnp.dot(weights.astype(bf16), kv_here, preferred_element_type=f32)
        if i:
            weights = jnp.exp(past - best)
            total = total + jnp.sum(weights, axis=1, keepdims=True)
            value = value + jnp.dot(weights.astype(bf16), kv_past, preferred_element_type=f32)
        value = value / total
        if packed:
            value = jnp.where(key_lanes, swap(value[short:]), value[:short])
        osend[i] = value.astype(bf16)

        @pl.when(s != i)
        def _():
            o_copy(i).start()

        @pl.when(s == i)
        def _():
            obuf[i] = osend[i]

    for d in range(1, sp):
        j = s ^ d
        remote(obuf.at[j], obuf.at[j], o_send.at[0], o_recv.at[j], j, t).wait_recv()
    low = low_lanes(short)
    for r in range(g):
        at = r * piece
        if hpd == 1:
            attbuf[t, at:at + piece, :] = obuf[r][:, :HD]
        else:
            for p in range(hpd // 2):
                pair = slice(p * LANES, (p + 1) * LANES)
                even = obuf[(2 * p) * g + r].astype(f32)
                odd = obuf[(2 * p + 1) * g + r].astype(f32)
                attbuf[t, at:at + short, pair] = jnp.where(low, even, odd).astype(bf16)
                if packed:
                    attbuf[t, at + short:at + piece, pair] = swap(jnp.where(low, odd, even)).astype(bf16)

    def ay_copy(k):
        at = attbuf.at[t]
        return remote(at, at, ay_send.at[k], a_recv.at[t], s, t ^ (2 * k))

    def ap_copy(k):
        a = t ^ (2 * k)
        at = attbuf.at[a]
        return remote(at, at, ap_send.at[k], a_recv.at[a], s, t ^ 1)

    def a_arrival(a):
        at = attbuf.at[a]
        return remote(at, at, ap_send.at[0], a_recv.at[a], s, t ^ 1)

    for k in range(1, ny):
        ay_copy(k).start()
    ap_copy(0).start()
    for k in range(1, ny):
        a_arrival(t ^ (2 * k)).wait_recv()
        ap_copy(k).start()
    own_w.wait()
    own_resid.wait()
    for a in range(1, tp):
        remote(wbuf.at[t ^ a], wbuf.at[t ^ a], w_send.at[0], w_recv.at[t ^ a], s, t ^ 1).wait_recv()
    for k in range(ny):
        a_arrival(t ^ (2 * k + 1)).wait_recv()
    mixed = resbuf[...].astype(f32)
    for a in range(tp):
        mixed = mixed + jnp.dot(attbuf[a], wbuf[a], preferred_element_type=f32)
    stream[...] = mixed
    square = jnp.sum(mixed * mixed, axis=1, keepdims=True)
    sums[t] = jnp.sum(jnp.where(along == across, square, 0.0), axis=0, keepdims=True)

    def n_copy(a):
        return remote(sums.at[t], sums.at[t], n_send.at[a], n_recv.at[t], s, t ^ a)

    for a in range(1, tp):
        n_copy(a).start()
    for a in range(1, tp):
        at = sums.at[t ^ a]
        remote(at, at, n_send.at[0], n_recv.at[t ^ a], s, t ^ 1).wait_recv()
    square = sums[0]
    for a in range(1, tp):
        square = square + sums[a]
    scale = lax.rsqrt(square / width + EPSILON)
    scale = jnp.sum(jnp.where(along == across, scale, 0.0), axis=1, keepdims=True)
    resbuf[...] = (stream[...] * scale * gain_ref[:, window(t)]).astype(bf16)

    def x_copy(d):
        return remote(
            rows.at[d], gath.at[d, :, window(t)], x_send.at[d], x_recv.at[d], s ^ d, t
        )

    def y_copy(d, k):
        at = gath.at[d, :, window(t)]
        return remote(at, at, gy_send.at[d, k], g_recv.at[d, t], s, t ^ (2 * k))

    def p_copy(d, k):
        a = t ^ (2 * k)
        at = gath.at[d, :, window(a)]
        return remote(at, at, gp_send.at[d, k], g_recv.at[d, a], s, t ^ 1)

    def arrival(d, a):
        at = gath.at[d, :, window(a)]
        return remote(at, at, gp_send.at[d, 0], g_recv.at[d, a], s, t ^ 1)

    def forward(d):
        if d:
            x_copy(d).wait_recv()
        for k in range(1, ny):
            y_copy(d, k).start()
        p_copy(d, 0).start()

    def relay(d):
        for k in range(1, ny):
            arrival(d, t ^ (2 * k)).wait_recv()
            p_copy(d, k).start()

    def finish(d):
        for k in range(ny):
            arrival(d, t ^ (2 * k + 1)).wait_recv()

    def send(d, n):
        out = jnp.dot(pick[d * slots:(d + n) * slots, :], resbuf[...], preferred_element_type=f32).astype(bf16)
        for j in range(n):
            block = out[j * slots:(j + 1) * slots]
            if d + j:
                rows[d + j] = block
                x_copy(d + j).start()
            else:
                gath[0, :, window(t)] = block
                forward(0)

    late = 3 * sp // 8 * 2
    for d in range(0, late, 2):
        send(d, 2)
    forward(1)
    relay(0)
    forward(2)
    for d in range(late, sp, 2):
        send(d, 2)
    relay(1)
    forward(3)

    def ps_copy(d, k):
        return remote(psend.at[d, k], precv.at[d, k], ps_send.at[d, k], ps_recv.at[d, k], s, t ^ 1)

    def ys_copy(d, k):
        return remote(ysend.at[d, k], yrecv.at[d, k], ys_send.at[d, k], ys_recv.at[d, k], s, t ^ (2 * k))

    def r_copy(d, place=0):
        at = ret.at[pl.ds(place * slots, slots)]
        return remote(erows.at[d], at, r_send.at[d], r_recv.at[d], s ^ d, t)

    def gate_up(d, n, tiles):
        x = gath[d:d + n].reshape(n * slots, width)
        for j in tiles:
            at = slice(j * tile, (j + 1) * tile)
            gate = jnp.dot(x, wg[:, at], preferred_element_type=f32)
            up = jnp.dot(x, wu[:, at], preferred_element_type=f32)
            hid[:n * slots, at] = (gate / (1.0 + jnp.exp(-gate)) * up).astype(bf16)

    order = list(range(1, ny)) + [0]

    def block(n, b):
        return jnp.dot(hid[:n * slots, :], wd[:, window(b)], preferred_element_type=f32)

    def down_pair(d, n):
        for k in order:
            out = block(n, t ^ (2 * k + 1)).astype(bf16)
            for j in range(n):
                psend[d + j, k] = out[j * slots:(j + 1) * slots]
                ps_copy(d + j, k).start()

    def down_own(d, n):
        for k in order:
            out = block(n, t ^ (2 * k))
            for j in range(n):
                part[d + j, k] = out[j * slots:(j + 1) * slots]

    def add_pair(d, n):
        for k in order:
            for j in range(n):
                ps_copy(d + j, k).wait_recv()
                total = part[d + j, k] + precv[d + j, k].astype(f32)
                if k:
                    ysend[d + j, k] = total.astype(bf16)
                    ys_copy(d + j, k).start()
                else:
                    part[d + j, k] = total

    def give_back(d, n):
        for j in range(d, d + n):
            total = part[j, 0]
            for k in range(1, ny):
                ys_copy(j, k).wait_recv()
                total = total + yrecv[j, k].astype(f32)
            erows[j] = total.astype(bf16)
            if j:
                r_copy(j, places.index(j)).start()

    tiles = range(units // tile)
    for n, d in enumerate(plan):
        finish(d)
        finish(d + 1)
        if not n:
            for load in loads:
                load.wait()
        gate_up(d, 2, tiles)
        if not n:
            forward(4)
        down_pair(d, 2)
        if not n:
            forward(5)
        down_own(d, 2)
        if n > 1:
            give_back(plan[n - 1], 2)
        add_pair(d, 2)
        if n == 1:
            give_back(plan[0], 2)
        if not n:
            relay(2)
            relay(3)
        if n + 3 < len(plan):
            forward(plan[n + 2])
            forward(plan[n + 2] + 1)
        if n + 2 < len(plan):
            relay(plan[n + 1])
            relay(plan[n + 1] + 1)
    give_back(plan[-1], 2)

    ret[:slots] = erows[0]
    for n in range(1, sp):
        r_copy(places[n], n).wait_recv()
    back = ret[...]
    combined = jnp.dot(share[0], back, preferred_element_type=f32)
    combined = combined + jnp.dot(share[1], back, preferred_element_type=f32)
    combined = stream[...] + combined
    out_ref[...] = combined.astype(bf16)

    for d in range(1, sp):
        q_copy(d).wait_send()
        if d % 2 == 0:
            kv_copy(d).wait_send()
            kv_pass(d).wait_send()
    kv_pass(0).wait_send()
    for i in range(sp):
        @pl.when(s != i)
        def _():
            o_copy(i).wait_send()
    for a in range(1, tp):
        w_copy(a).wait_send()
        n_copy(a).wait_send()
    for k in range(ny):
        ap_copy(k).wait_send()
        if k:
            ay_copy(k).wait_send()

    def drain(d, carry):
        @pl.when(d > 0)
        def _():
            x_copy(d).wait_send()
            r_copy(d).wait_send()

        for k in range(ny):
            p_copy(d, k).wait_send()
            ps_copy(d, k).wait_send()
            if k:
                y_copy(d, k).wait_send()
                ys_copy(d, k).wait_send()
        return carry

    lax.fori_loop(0, sp, drain, 0)


def local(
    queries, keys, values, cum_gate, out_weight, resid, norm_gain, routes, route_weight,
    gate_weight, up_weight, down_weight,
):
    tokens = queries.shape[0]
    hpd = queries.shape[1] // HD
    sp, tp = lax.axis_size("sp"), lax.axis_size("tp")
    width = resid.shape[1]
    cols = width // tp
    units = gate_weight.shape[2]
    tile = min(256, units)
    piece = tokens // (sp // hpd)
    short = piece // 2 if hpd > 1 and piece % 32 == 0 else piece
    cap = 5 * tokens // (2 * sp)
    slots = -(-cap // 16) * 16
    ny = tp // 2
    bf16, f32 = jnp.bfloat16, jnp.float32
    dma = pltpu.SemaphoreType.DMA

    def vm(*shape, dtype=bf16):
        return pltpu.VMEM(shape, dtype)

    vmem = pl.BlockSpec(memory_space=pltpu.VMEM)
    anywhere = pl.BlockSpec(memory_space=pl.ANY)
    return pl.pallas_call(
        functools.partial(layer_kernel, sp, tp, hpd, slots, tile),
        out_shape=jax.ShapeDtypeStruct((tokens, cols), bf16),
        in_specs=[vmem] * 7 + [anywhere] * 5,
        out_specs=vmem,
        scratch_shapes=[
            vm(hpd, tokens, LANES), vm(sp, tokens, LANES),
            vm(sp, short, LANES), vm(sp, short, LANES), vm(sp, short, LANES), vm(sp, short, LANES),
            vm(1, sp * tokens, dtype=f32), vm(sp, piece, 1, dtype=f32),
            vm(hpd * HD, width), vm(tp, hpd * HD, cols), vm(tp, tokens, hpd * HD), vm(tokens, cols),
            vm(tokens, cols, dtype=f32), vm(tp, 1, tokens, dtype=f32),
            vm(sp * slots, tokens), vm(2, tokens, sp * slots),
            vm(sp, slots, cols), vm(sp, slots, width),
            vm(width, units), vm(width, units), vm(units, width), vm(2 * slots, units),
            vm(sp, ny, slots, cols), vm(sp, ny, slots, cols), vm(sp, ny, slots, cols, dtype=f32),
            vm(sp, ny, slots, cols), vm(sp, ny, slots, cols), vm(sp, slots, cols), vm(sp * slots, cols),
            dma((3,)), dma((3,)), dma((sp,)), dma((sp,)), dma((sp,)), dma((sp,)), dma((sp,)),
            dma((sp,)), dma((sp,)),
            dma((tp,)), dma((tp,)), dma((ny,)), dma((ny,)), dma((tp,)), dma((tp,)), dma((tp,)),
            dma((sp,)), dma((sp,)), dma((sp, ny)), dma((sp, ny)), dma((sp, tp)),
            dma((sp, ny)), dma((sp, ny)), dma((sp, ny)), dma((sp, ny)), dma((sp,)), dma((sp,)),
        ],
        compiler_params=pltpu.CompilerParams(
            collective_id=0, has_side_effects=True, vmem_limit_bytes=VMEM_BYTES
        ),
        name="layer",
    )(
        queries, keys, values, cum_gate, norm_gain[None, :], routes.T, route_weight.T,
        out_weight, resid, gate_weight, up_weight, down_weight,
    )


def solution(mesh):
    return jax.shard_map(
        local,
        mesh=mesh,
        in_specs=(
            P("sp", "tp"), P("sp", "tp"), P("sp", "tp"), P("tp", None), P("tp", None), P("sp", None),
            P(), P("sp", None), P("sp", None), P("sp", None, "tp"), P("sp", None, "tp"), P("sp", "tp", None),
        ),
        out_specs=P("sp", "tp"),
        check_vma=False,
    )
```

```python
import functools

import jax
import jax.numpy as jnp
from jax import lax
from jax.experimental import pallas as pl
from jax.experimental.pallas import tpu as pltpu
from jax.sharding import PartitionSpec as P

HD = 64
LANES = 128
EPSILON = 1e-06
MESH = pl.DeviceIdType.MESH
VMEM_BYTES = 60 * 1024 * 1024
CONTRACT_LAST = (((1,), (1,)), ((), ()))


def remote(src, dst, send_sem, recv_sem, s, t):
    return pltpu.make_async_remote_copy(
        src_ref=src,
        dst_ref=dst,
        send_sem=send_sem,
        recv_sem=recv_sem,
        device_id=(s, t),
        device_id_type=MESH,
    )


def layer_kernel(
    sp, tp, hpd, slots, tile,
    q_ref, k_ref, v_ref, cum_ref, gain_ref, routes_ref, share_ref,
    w_ref, resid_ref, wg_ref, wu_ref, wd_ref,
    out_ref,
    kvs, kvbuf, qs, qbuf, osend, obuf, ckb, cqb, wsrc, wbuf, attbuf, resbuf, stream, sums, pick, share,
    rows, gath, wg, wu, wd, hid, psend, precv, part, ysend, yrecv, erows, ret,
    local_sem, load_sem, kv_send, kv_relay, kv_recv, q_send, q_recv, o_send, o_recv,
    w_send, w_recv, ay_send, ap_send, a_recv, n_send, n_recv,
    x_send, x_recv, gy_send, gp_send, g_recv, ps_send, ps_recv, ys_send, ys_recv, r_send, r_recv,
):
    f32, bf16 = jnp.float32, jnp.bfloat16
    s, t = lax.axis_index("sp"), lax.axis_index("tp")
    ny = tp // 2
    g = sp // hpd
    tokens = q_ref.shape[0]
    piece = tokens // g
    packed = qs.shape[1] < piece
    short = qs.shape[1]
    width = gath.shape[2]
    cols = width // tp
    units = hid.shape[1]

    def window(a):
        return pl.ds(pl.multiple_of(a * cols, cols), cols)

    own_w = pltpu.make_async_copy(w_ref.at[:, window(t)], wbuf.at[t], local_sem.at[0])
    all_w = pltpu.make_async_copy(w_ref, wsrc, local_sem.at[2])
    own_resid = pltpu.make_async_copy(resid_ref.at[:, window(t)], resbuf, local_sem.at[1])
    loads = [
        pltpu.make_async_copy(src.at[0], dst, load_sem.at[i])
        for i, (src, dst) in enumerate(((wg_ref, wg), (wu_ref, wu), (wd_ref, wd)))
    ]

    barrier = pltpu.get_barrier_semaphore()
    for d in range(1, sp):
        pl.semaphore_signal(barrier, inc=1, device_id=(s ^ d, t), device_id_type=MESH)
    for a in range(1, tp):
        pl.semaphore_signal(barrier, inc=1, device_id=(s, t ^ a), device_id_type=MESH)
    all_w.start()
    own_w.start()
    own_resid.start()

    def swap(x):
        return jnp.concatenate([x[:, HD:], x[:, :HD]], axis=1)

    def low_lanes(n):
        return lax.broadcasted_iota(jnp.int32, (n, LANES), 1) < HD

    if hpd == 1:
        kvs[0] = jnp.concatenate([v_ref[...], k_ref[...]], axis=1)
        q = q_ref[...].astype(f32) * HD ** -0.5
        q = jnp.concatenate([jnp.zeros_like(q), q], axis=1).astype(bf16)
        for j in range(sp):
            qs[j] = q[j * piece:(j + 1) * piece]
    else:
        low = low_lanes(tokens)
        for p in range(hpd // 2):
            pair = slice(p * LANES, (p + 1) * LANES)
            k = swap(k_ref[:, pair].astype(f32))
            v = v_ref[:, pair].astype(f32)
            kvs[2 * p] = jnp.where(low, v, k).astype(bf16)
            kvs[2 * p + 1] = jnp.where(low, k, v).astype(bf16)
            q = q_ref[:, pair].astype(f32) * HD ** -0.5
            turned = swap(q)
            for odd in range(2):
                for r in range(g):
                    at = r * piece
                    front = turned[at:at + short]
                    back = q[at + short:at + piece] if packed else jnp.zeros_like(front)
                    keys_low = low_lanes(short)
                    both = jnp.where(keys_low, front, back) if odd else jnp.where(keys_low, back, front)
                    qs[(2 * p + odd) * g + r] = both.astype(bf16)
    pl.semaphore_wait(barrier, sp + tp - 2)

    def kv_copy(d):
        dst = s ^ d
        return remote(kvs.at[dst // g], kvbuf.at[s], kv_send.at[d], kv_recv.at[s], dst, t)

    def kv_pass(d):
        i = s ^ d
        src = kvbuf.at[i] if d else kvs.at[s // g]
        return remote(src, kvbuf.at[i], kv_relay.at[d], kv_recv.at[i], s ^ 1, t)

    def kv_arrival(i):
        return remote(kvbuf.at[i], kvbuf.at[i], kv_relay.at[0], kv_recv.at[i], s ^ 1, t)

    def q_copy(d):
        dst = s ^ d
        return remote(qs.at[dst], qbuf.at[s], q_send.at[d], q_recv.at[s], dst, t)

    def w_copy(a):
        return remote(wsrc.at[:, window(t ^ a)], wbuf.at[t], w_send.at[a], w_recv.at[t], s, t ^ a)

    for d in range(2, sp, 2):
        kv_copy(d).start()
    kv_pass(0).start()
    all_w.wait()
    for a in range(1, tp):
        w_copy(a).start()
    for load in loads:
        load.start()
    kvbuf[s] = kvs[s // g]
    qbuf[s] = qs[s]

    head = s // g
    first = lax.rem(s, g) * piece
    qpos = first + lax.broadcasted_iota(jnp.int32, (piece, tokens), 0)
    kpos = lax.broadcasted_iota(jnp.int32, (piece, tokens), 1)
    ckb[...] = cum_ref[pl.ds(head, 1), :]
    for i in range(sp):
        here = ckb[:, i * tokens:(i + 1) * tokens]
        cqb[i] = jnp.sum(jnp.where(kpos == qpos, here, 0.0), axis=1, keepdims=True)
    experts = lax.broadcasted_iota(jnp.int32, (sp, tokens), 0) ^ s
    chosen = [routes_ref[k:k + 1, :] == experts for k in range(2)]
    named = jnp.where(chosen[0] | chosen[1], 1.0, 0.0)
    weight = sum(jnp.where(chosen[k], share_ref[k:k + 1, :], 0.0) for k in range(2))
    high = weight.astype(bf16).astype(f32)
    parts = (high, weight - high)
    across = lax.broadcasted_iota(jnp.int32, (tokens, tokens), 1)
    along = lax.broadcasted_iota(jnp.int32, (tokens, tokens), 0)
    before = jnp.where(along < across, 1.0, 0.0).astype(bf16)
    rank = jnp.dot(named.astype(bf16), before, preferred_element_type=f32)
    rank = jnp.where(named > 0.0, rank, -1.0)
    slot = lax.broadcasted_iota(jnp.int32, (slots, tokens), 0).astype(f32)
    shares = ([], [])
    plan = [0] + list(range(4, sp, 2)) + [2]
    places = [d + j for d in plan for j in range(2)]
    for d in places:
        taken = slot == rank[d:d + 1, :]
        pick[d * slots:(d + 1) * slots, :] = jnp.where(taken, 1.0, 0.0).astype(bf16)
        for n in range(2):
            shares[n].append(jnp.where(taken, parts[n][d:d + 1, :], 0.0))
    for n in range(2):
        share[n] = jnp.concatenate(shares[n], axis=0).T.astype(bf16)

    for d in range(2, sp, 2):
        kv_arrival(s ^ d).wait_recv()
        kv_pass(d).start()
        if d == 2:
            for j in range(sp - 1, 0, -1):
                q_copy(j).start()

    def o_copy(i):
        return remote(osend.at[i], obuf.at[s], o_send.at[i], o_recv.at[s], i, t)

    half = lax.broadcasted_iota(jnp.int32, (short, LANES), 1) // HD
    key_lanes = (half + lax.rem(head, 2)) == 1
    for i in range(sp):
        @pl.when(s != i)
        def _():
            remote(qbuf.at[i], qbuf.at[i], q_send.at[0], q_recv.at[i], s ^ 1, t).wait_recv()

        @pl.when((s != i) & (lax.rem(s + i, 2) == 1))
        def _():
            kv_arrival(i).wait_recv()

        q = qbuf[i]
        if packed:
            q = q.astype(f32)
            q = jnp.concatenate(
                [jnp.where(key_lanes, q, 0.0), jnp.where(key_lanes, swap(q), 0.0)], axis=0
            ).astype(bf16)
        cq = cqb[i]
        kv_here = kvbuf[i]
        diag = lax.dot_general(q, kv_here, CONTRACT_LAST, preferred_element_type=f32)
        diag = diag + cq - ckb[:, i * tokens:(i + 1) * tokens]
        diag = jnp.where(kpos <= qpos, diag, -jnp.inf)
        best = jnp.max(diag, axis=1, keepdims=True)
        if i:
            kv_past = kvbuf[0:i].reshape(i * tokens, LANES)
            past = lax.dot_general(q, kv_past, CONTRACT_LAST, preferred_element_type=f32)
            past = past + cq - ckb[:, :i * tokens]
            best = jnp.maximum(best, jnp.max(past, axis=1, keepdims=True))
        weights = jnp.exp(diag - best)
        total = jnp.sum(weights, axis=1, keepdims=True)
        value = jnp.dot(weights.astype(bf16), kv_here, preferred_element_type=f32)
        if i:
            weights = jnp.exp(past - best)
            total = total + jnp.sum(weights, axis=1, keepdims=True)
            value = value + jnp.dot(weights.astype(bf16), kv_past, preferred_element_type=f32)
        value = value / total
        if packed:
            value = jnp.where(key_lanes, swap(value[short:]), value[:short])
        osend[i] = value.astype(bf16)

        @pl.when(s != i)
        def _():
            o_copy(i).start()

        @pl.when(s == i)
        def _():
            obuf[i] = osend[i]

    for d in range(1, sp):
        j = s ^ d
        remote(obuf.at[j], obuf.at[j], o_send.at[0], o_recv.at[j], j, t).wait_recv()
    low = low_lanes(short)
    for r in range(g):
        at = r * piece
        if hpd == 1:
            attbuf[t, at:at + piece, :] = obuf[r][:, :HD]
        else:
            for p in range(hpd // 2):
                pair = slice(p * LANES, (p + 1) * LANES)
                even = obuf[(2 * p) * g + r].astype(f32)
                odd = obuf[(2 * p + 1) * g + r].astype(f32)
                attbuf[t, at:at + short, pair] = jnp.where(low, even, odd).astype(bf16)
                if packed:
                    attbuf[t, at + short:at + piece, pair] = swap(jnp.where(low, odd, even)).astype(bf16)

    def ay_copy(k):
        at = attbuf.at[t]
        return remote(at, at, ay_send.at[k], a_recv.at[t], s, t ^ (2 * k))

    def ap_copy(k):
        a = t ^ (2 * k)
        at = attbuf.at[a]
        return remote(at, at, ap_send.at[k], a_recv.at[a], s, t ^ 1)

    def a_arrival(a):
        at = attbuf.at[a]
        return remote(at, at, ap_send.at[0], a_recv.at[a], s, t ^ 1)

    for k in range(1, ny):
        ay_copy(k).start()
    ap_copy(0).start()
    for k in range(1, ny):
        a_arrival(t ^ (2 * k)).wait_recv()
        ap_copy(k).start()
    own_w.wait()
    own_resid.wait()
    for a in range(1, tp):
        remote(wbuf.at[t ^ a], wbuf.at[t ^ a], w_send.at[0], w_recv.at[t ^ a], s, t ^ 1).wait_recv()
    for k in range(ny):
        a_arrival(t ^ (2 * k + 1)).wait_recv()
    mixed = resbuf[...].astype(f32)
    for a in range(tp):
        mixed = mixed + jnp.dot(attbuf[a], wbuf[a], preferred_element_type=f32)
    stream[...] = mixed
    square = jnp.sum(mixed * mixed, axis=1, keepdims=True)
    sums[t] = jnp.sum(jnp.where(along == across, square, 0.0), axis=0, keepdims=True)

    def n_copy(a):
        return remote(sums.at[t], sums.at[t], n_send.at[a], n_recv.at[t], s, t ^ a)

    for a in range(1, tp):
        n_copy(a).start()
    for a in range(1, tp):
        at = sums.at[t ^ a]
        remote(at, at, n_send.at[0], n_recv.at[t ^ a], s, t ^ 1).wait_recv()
    square = sums[0]
    for a in range(1, tp):
        square = square + sums[a]
    scale = lax.rsqrt(square / width + EPSILON)
    scale = jnp.sum(jnp.where(along == across, scale, 0.0), axis=1, keepdims=True)
    resbuf[...] = (stream[...] * scale * gain_ref[:, window(t)]).astype(bf16)

    def x_copy(d):
        return remote(
            rows.at[d], gath.at[d, :, window(t)], x_send.at[d], x_recv.at[d], s ^ d, t
        )

    def y_copy(d, k):
        at = gath.at[d, :, window(t)]
        return remote(at, at, gy_send.at[d, k], g_recv.at[d, t], s, t ^ (2 * k))

    def p_copy(d, k):
        a = t ^ (2 * k)
        at = gath.at[d, :, window(a)]
        return remote(at, at, gp_send.at[d, k], g_recv.at[d, a], s, t ^ 1)

    def arrival(d, a):
        at = gath.at[d, :, window(a)]
        return remote(at, at, gp_send.at[d, 0], g_recv.at[d, a], s, t ^ 1)

    def forward(d):
        if d:
            x_copy(d).wait_recv()
        for k in range(1, ny):
            y_copy(d, k).start()
        p_copy(d, 0).start()

    def relay(d):
        for k in range(1, ny):
            arrival(d, t ^ (2 * k)).wait_recv()
            p_copy(d, k).start()

    def finish(d):
        for k in range(ny):
            arrival(d, t ^ (2 * k + 1)).wait_recv()

    def send(d, n):
        out = jnp.dot(pick[d * slots:(d + n) * slots, :], resbuf[...], preferred_element_type=f32).astype(bf16)
        for j in range(n):
            block = out[j * slots:(j + 1) * slots]
            if d + j:
                rows[d + j] = block
                x_copy(d + j).start()
            else:
                gath[0, :, window(t)] = block
                forward(0)

    late = 3 * sp // 8 * 2
    for d in range(0, late, 2):
        send(d, 2)
    forward(1)
    relay(0)
    forward(2)
    for d in range(late, sp, 2):
        send(d, 2)
    relay(1)
    forward(3)

    def ps_copy(d, k):
        return remote(psend.at[d, k], precv.at[d, k], ps_send.at[d, k], ps_recv.at[d, k], s, t ^ 1)

    def ys_copy(d, k):
        return remote(ysend.at[d, k], yrecv.at[d, k], ys_send.at[d, k], ys_recv.at[d, k], s, t ^ (2 * k))

    def r_copy(d, place=0):
        at = ret.at[pl.ds(place * slots, slots)]
        return remote(erows.at[d], at, r_send.at[d], r_recv.at[d], s ^ d, t)

    def gate_up(d, n, tiles):
        x = gath[d:d + n].reshape(n * slots, width)
        for j in tiles:
            at = slice(j * tile, (j + 1) * tile)
            gate = jnp.dot(x, wg[:, at], preferred_element_type=f32)
            up = jnp.dot(x, wu[:, at], preferred_element_type=f32)
            hid[:n * slots, at] = (gate / (1.0 + jnp.exp(-gate)) * up).astype(bf16)

    order = list(range(1, ny)) + [0]

    def block(n, b):
        return jnp.dot(hid[:n * slots, :], wd[:, window(b)], preferred_element_type=f32)

    def down_pair(d, n):
        for k in order:
            out = block(n, t ^ (2 * k + 1)).astype(bf16)
            for j in range(n):
                psend[d + j, k] = out[j * slots:(j + 1) * slots]
                ps_copy(d + j, k).start()

    def down_own(d, n):
        for k in order:
            out = block(n, t ^ (2 * k))
            for j in range(n):
                part[d + j, k] = out[j * slots:(j + 1) * slots]

    def add_pair(d, n):
        for k in order:
            for j in range(n):
                ps_copy(d + j, k).wait_recv()
                total = part[d + j, k] + precv[d + j, k].astype(f32)
                if k:
                    ysend[d + j, k] = total.astype(bf16)
                    ys_copy(d + j, k).start()
                else:
                    part[d + j, k] = total

    def give_back(d, n):
        for j in range(d, d + n):
            total = part[j, 0]
            for k in range(1, ny):
                ys_copy(j, k).wait_recv()
                total = total + yrecv[j, k].astype(f32)
            erows[j] = total.astype(bf16)
            if j:
                r_copy(j, places.index(j)).start()

    tiles = range(units // tile)
    for n, d in enumerate(plan):
        finish(d)
        finish(d + 1)
        if not n:
            for load in loads:
                load.wait()
        gate_up(d, 2, tiles)
        if not n:
            forward(4)
        down_pair(d, 2)
        if not n:
            forward(5)
        down_own(d, 2)
        if n > 1:
            give_back(plan[n - 1], 2)
        add_pair(d, 2)
        if n == 1:
            give_back(plan[0], 2)
        if not n:
            relay(2)
            relay(3)
        if n + 3 < len(plan):
            forward(plan[n + 2])
            forward(plan[n + 2] + 1)
        if n + 2 < len(plan):
            relay(plan[n + 1])
            relay(plan[n + 1] + 1)
    give_back(plan[-1], 2)

    ret[:slots] = erows[0]
    for n in range(1, sp):
        r_copy(places[n], n).wait_recv()
    back = ret[...]
    combined = jnp.dot(share[0], back, preferred_element_type=f32)
    combined = combined + jnp.dot(share[1], back, preferred_element_type=f32)
    combined = stream[...] + combined
    out_ref[...] = combined.astype(bf16)

    for d in range(1, sp):
        q_copy(d).wait_send()
        if d % 2 == 0:
            kv_copy(d).wait_send()
            kv_pass(d).wait_send()
    kv_pass(0).wait_send()
    for i in range(sp):
        @pl.when(s != i)
        def _():
            o_copy(i).wait_send()
    for a in range(1, tp):
        w_copy(a).wait_send()
        n_copy(a).wait_send()
    for k in range(ny):
        ap_copy(k).wait_send()
        if k:
            ay_copy(k).wait_send()

    def drain(d, carry):
        @pl.when(d > 0)
        def _():
            x_copy(d).wait_send()
            r_copy(d).wait_send()

        for k in range(ny):
            p_copy(d, k).wait_send()
            ps_copy(d, k).wait_send()
            if k:
                y_copy(d, k).wait_send()
                ys_copy(d, k).wait_send()
        return carry

    lax.fori_loop(0, sp, drain, 0)


def local(
    queries, keys, values, cum_gate, out_weight, resid, norm_gain, routes, route_weight,
    gate_weight, up_weight, down_weight,
):
    tokens = queries.shape[0]
    hpd = queries.shape[1] // HD
    sp, tp = lax.axis_size("sp"), lax.axis_size("tp")
    width = resid.shape[1]
    cols = width // tp
    units = gate_weight.shape[2]
    tile = min(256, units)
    piece = tokens // (sp // hpd)
    short = piece // 2 if hpd > 1 and piece % 32 == 0 else piece
    cap = 5 * tokens // (2 * sp)
    slots = -(-cap // 16) * 16
    ny = tp // 2
    bf16, f32 = jnp.bfloat16, jnp.float32
    dma = pltpu.SemaphoreType.DMA

    def vm(*shape, dtype=bf16):
        return pltpu.VMEM(shape, dtype)

    vmem = pl.BlockSpec(memory_space=pltpu.VMEM)
    anywhere = pl.BlockSpec(memory_space=pl.ANY)
    return pl.pallas_call(
        functools.partial(layer_kernel, sp, tp, hpd, slots, tile),
        out_shape=jax.ShapeDtypeStruct((tokens, cols), bf16),
        in_specs=[vmem] * 7 + [anywhere] * 5,
        out_specs=vmem,
        scratch_shapes=[
            vm(hpd, tokens, LANES), vm(sp, tokens, LANES),
            vm(sp, short, LANES), vm(sp, short, LANES), vm(sp, short, LANES), vm(sp, short, LANES),
            vm(1, sp * tokens, dtype=f32), vm(sp, piece, 1, dtype=f32),
            vm(hpd * HD, width), vm(tp, hpd * HD, cols), vm(tp, tokens, hpd * HD), vm(tokens, cols),
            vm(tokens, cols, dtype=f32), vm(tp, 1, tokens, dtype=f32),
            vm(sp * slots, tokens), vm(2, tokens, sp * slots),
            vm(sp, slots, cols), vm(sp, slots, width),
            vm(width, units), vm(width, units), vm(units, width), vm(2 * slots, units),
            vm(sp, ny, slots, cols), vm(sp, ny, slots, cols), vm(sp, ny, slots, cols, dtype=f32),
            vm(sp, ny, slots, cols), vm(sp, ny, slots, cols), vm(sp, slots, cols), vm(sp * slots, cols),
            dma((3,)), dma((3,)), dma((sp,)), dma((sp,)), dma((sp,)), dma((sp,)), dma((sp,)),
            dma((sp,)), dma((sp,)),
            dma((tp,)), dma((tp,)), dma((ny,)), dma((ny,)), dma((tp,)), dma((tp,)), dma((tp,)),
            dma((sp,)), dma((sp,)), dma((sp, ny)), dma((sp, ny)), dma((sp, tp)),
            dma((sp, ny)), dma((sp, ny)), dma((sp, ny)), dma((sp, ny)), dma((sp,)), dma((sp,)),
        ],
        compiler_params=pltpu.CompilerParams(
            collective_id=0, has_side_effects=True, vmem_limit_bytes=VMEM_BYTES
        ),
        name="layer",
    )(
        queries, keys, values, cum_gate, norm_gain[None, :], routes.T, route_weight.T,
        out_weight, resid, gate_weight, up_weight, down_weight,
    )


def solution(mesh):
    return jax.shard_map(
        local,
        mesh=mesh,
        in_specs=(
            P("sp", "tp"), P("sp", "tp"), P("sp", "tp"), P("tp", None), P("tp", None), P("sp", None),
            P(), P("sp", None), P("sp", None), P("sp", None, "tp"), P("sp", None, "tp"), P("sp", "tp", None),
        ),
        out_specs=P("sp", "tp"),
        check_vma=False,
    )
```
